256 devices in a mesh: grp: 2 (over y), ep: 32 (over z, core), tp: 4 (over x).
Axes of the slice: x: 4, y: 2, z: 16, core: 2. Of those that a mesh axis runs over, the one named last changes fastest.
The devices are a block of a 4x16x16 slice.
Arguments:
- queries: bfloat16 [8192, 16, 128], P(('grp', 'ep'), 'tp'), parts along dimension 0, may hold values from -6 to 6
- key_vectors: bfloat16 [8192, 16, 128], P(('grp', 'ep'), 'tp'), parts along dimension 0, may hold values from -6 to 6
- values: bfloat16 [8192, 16, 128], P(('grp', 'ep'), 'tp'), parts along dimension 0, may hold values from -6 to 6
- forget_cum: float32 [8192, 16], P('grp', 'tp'), parts along dimension 0, may hold values from -699 to 0, as said below
- query_gain: float32 [128], replicated, may hold values from 0.1 to 5.5
- key_gain: float32 [128], replicated, may hold values from 0.1 to 5.5
- tokens: bfloat16 [32768, 4096], P(('grp', 'ep', 'tp')), parts along dimension 0, may hold values from -6 to 6
- norm_gain: float32 [4096], replicated, may hold values from 0.1 to 1.9
- routes: int32 [32768, 2], P(('grp', 'ep', 'tp')), parts along dimension 0, may hold values from 0 to 127, all different within a row; in each aligned block of 128 rows (0 to 127, 128 to 255, ...) at most 2 rows name the same one
- route_weights: float32 [32768, 2], P(('grp', 'ep', 'tp')), parts along dimension 0, may hold values from 0.3 to 1.2
- expert_gate: bfloat16 [128, 4096, 384], P(('ep', 'tp')), may hold values from -0.09375 to 0.09375
- expert_up: bfloat16 [128, 4096, 384], P(('ep', 'tp')), may hold values from -0.09375 to 0.09375
- expert_down: bfloat16 [128, 384, 4096], P(('ep', 'tp')), may hold values from -0.3125 to 0.3125
- shared_gate: bfloat16 [4096, 192], P(None, 'tp'), may hold values from -0.09375 to 0.09375
- shared_up: bfloat16 [4096, 192], P(None, 'tp'), may hold values from -0.09375 to 0.09375
- shared_down: bfloat16 [192, 4096], P('tp'), may hold values from -0.4375 to 0.4375
Outputs:
- attended: bfloat16 [8192, 16, 128], P(('grp', 'ep'), 'tp'), parts along dimension 0
- routed_output: bfloat16 [32768, 4096], P(('grp', 'ep', 'tp')), parts along dimension 0
The draws below stay inside these ranges and needn't reach their ends.
There are 2 independent parts, one for each index of `grp`. The reference program is written for one: setup_inputs(seed, part) draws one part's arguments, and reference() takes and returns one part's arrays. A program takes and returns all parts, laid end to end along the dimension named above; an argument that names none is the same for every part. Nothing has to cross between parts.
Inputs may be any that keep to these rules, and one draw needn't show every extreme that they name: `routes`: each row names 2 different experts; the rows of one device name every expert exactly 2 times. `forget_cum`: never rises from one position to the next.
All inputs are finite; a program needn't handle non-finite values.
Results may differ from the reference program's by a relative error of at most 0.007.
The reference program's roundings to bfloat16 on the way count: a program that leaves them out, or rounds other values in their place, can miss the bound.
Values may be sent and summed in bfloat16 or wider, within the bound.
A program may use at most 128 MiB of HBM per device.

```python
import math
import jax
import jax.numpy as jnp
import numpy as np
from jax import lax

D = 4096
HEADS = 16
HD = 128
EXPERTS = 128
EF = 384
SF = 192
TOP_K = 2
TOKENS_PER_SHARD = 128
TOK_B = 128
CAP = 2
SEQUENCE_LENGTH = 4096
TOKENS_B = 16384
N_EP = 32
N_TP = 4


def query_key_pair(key):
    query_base = jnp.clip(jax.random.normal(jax.random.fold_in(key, 701), (SEQUENCE_LENGTH, HEADS, HD), jnp.float32), -6.0, 6.0)
    key_base = jnp.clip(jax.random.normal(jax.random.fold_in(key, 702), (SEQUENCE_LENGTH, HEADS, HD), jnp.float32), -6.0, 6.0)
    return (query_base, key_base)


def draw_queries(key, part):
    return query_key_pair(key)[0].astype(jnp.bfloat16)


def draw_key_vectors(key, part):
    return query_key_pair(key)[1].astype(jnp.bfloat16)


def gain_sample(key):
    return 1.0 + jnp.clip(0.18 * jax.random.normal(key, (HD,), jnp.float32), -0.9, 0.9)


def draw_query_gain(key, part):
    return gain_sample(jax.random.fold_in(key, 801))


def draw_key_gain(key, part):
    return gain_sample(jax.random.fold_in(key, 802))


def draw_forget_cum(key, part):
    order = jax.random.permutation(jax.random.fold_in(key, 901), HEADS)
    gentle_decay = (order < HEADS // 2).astype(jnp.float32)
    totals = jnp.exp(jax.random.uniform(jax.random.fold_in(key, 902), (HEADS,), jnp.float32, jnp.log(0.3), jnp.log(1.0))) / SEQUENCE_LENGTH
    quick = jnp.exp(jax.random.uniform(jax.random.fold_in(key, 903), (HEADS,), jnp.float32, jnp.log(1.0 / 60.0), jnp.log(1.0 / 25.0)))
    decay_speed = gentle_decay * totals + (1.0 - gentle_decay) * quick
    block_multiplier = jnp.exp(jax.random.uniform(jax.random.fold_in(key, 904), (SEQUENCE_LENGTH // TOKENS_PER_SHARD,), jnp.float32, jnp.log(0.35), jnp.log(2.8)))
    jagged_profile = jax.random.uniform(jax.random.fold_in(key, 905), (SEQUENCE_LENGTH, HEADS), jnp.float32, 0.5, 1.5)
    position_indices = jnp.arange(SEQUENCE_LENGTH)
    spike_position = jax.random.randint(jax.random.fold_in(key, 906), (3,), 0, SEQUENCE_LENGTH)
    spike_magnitude = jax.random.uniform(jax.random.fold_in(key, 907), (3,), jnp.float32, 0.22, 0.69)
    forget_spike = jnp.sum(jnp.where(position_indices[:, None] == spike_position[None, :], spike_magnitude[None, :], 0.0), axis=1)
    forget_logarithm = -(decay_speed[None, :] * jnp.repeat(block_multiplier, TOKENS_PER_SHARD)[:, None] * jagged_profile) - forget_spike[:, None] * gentle_decay[None, :]
    return jnp.cumsum(forget_logarithm, axis=0)


def block_levels(stream_key, shape, shards, least, top_value):
    gain, own = 1.0, jax.random.fold_in(stream_key, 6)
    for dim, parts in shards:
        draws = jnp.exp(jax.random.uniform(jax.random.fold_in(own, dim), (parts,), jnp.float32, least / len(shards), top_value / len(shards)))
        gain = gain * jnp.repeat(draws, shape[dim] // parts).reshape([-1 if axis == dim else 1 for axis in range(len(shape))])
    return gain


def deal_out(own_key, own, number, rows, amount, top, most, lean):
    order = jax.random.permutation(own_key, amount)
    heavy_load, usual = portions_of(amount, rows * top, most, lean, True), portions_of(amount, rows * top, most, lean, False)
    places = jnp.arange(amount)

    def named(sizes, rotation):
        used = int((sizes > 0).sum())
        fixed = max(1, used // 4)
        passed = fixed + (places - fixed + rotation * (used - fixed)) % max(1, amount - fixed)
        return jnp.zeros((amount,), jnp.int32).at[order[jnp.where(places < fixed, places, passed)]].set(jnp.asarray(sizes, jnp.int32))

    sizes = jnp.where(number % 4 == 0, named(heavy_load, number // 4), named(usual, number - number // 4 - 1))
    mixed = jax.random.permutation(jax.random.fold_in(own, 3), amount)
    source_of, taker = mixed[0:amount // 2 * 2:2], mixed[1:amount // 2 * 2:2]
    margin = jnp.minimum(sizes[source_of] - 1, most - sizes[taker]) // 2
    margin = jnp.where((source_of == order[0]) | (taker == order[0]) | (sizes[taker] == 0), 0, jnp.maximum(margin, 0))
    passed = jax.random.randint(jax.random.fold_in(own, 4), (amount // 2,), 0, 1 << 20) % (margin + 1)
    sizes = sizes.at[source_of].add(-passed).at[taker].add(passed)
    items = jnp.searchsorted(jnp.cumsum(sizes), jnp.arange(rows * top), side="right").astype(jnp.int32)
    grid = items.reshape(top, rows).T
    grid = grid[jax.random.permutation(jax.random.fold_in(own, 1), rows)]
    rotation = jax.random.randint(jax.random.fold_in(own, 2), (rows, 1), 0, top)
    return jnp.take_along_axis(grid, (jnp.arange(top)[None, :] + rotation) % top, axis=1)


def portions_of(number_of, total, limit, skew, full):
    loads = [(1 << 20) // math.isqrt(grade ** skew) + 1 for grade in range(1, number_of + 1)]
    largest = limit if full else min(limit, max(-(-total // number_of), total * loads[0] // sum(loads)))
    least = 1 if total - largest >= number_of - 1 else 0
    counts, surplus = [largest] + [least] * (number_of - 1), total - largest - least * (number_of - 1)
    while surplus > 0:
        movable = [i for i in range(1, number_of) if counts[i] < largest] or [i for i in range(1, number_of) if counts[i] < limit]
        mass, budget = sum([loads[i] for i in movable]), surplus
        for i in movable:
            addition = min(limit - counts[i], max(1, budget * loads[i] // mass), surplus)
            counts[i] = counts[i] + addition
            surplus = surplus - addition
    return np.array(counts)


def scatter_about(key, dims, width, most, shards=(), held_as=jnp.bfloat16):
    level = block_levels(key, dims, shards, -0.22, 0.18) if shards else 1.0
    drawn = jax.random.normal(key, dims, jnp.float32) * width * level
    return jnp.minimum(jnp.maximum(drawn, -most), most).astype(held_as)


def setup_inputs(seed: int = 0, part: int = 0) -> dict:
    streams_of = jax.random.split(jax.random.key(seed), 17)
    part_keys = jax.random.split(jax.random.fold_in(streams_of[16], part), 17)
    queries = draw_queries(jax.random.fold_in(jax.random.fold_in(streams_of[16], part), 71), part)
    key_vectors = draw_key_vectors(jax.random.fold_in(jax.random.fold_in(streams_of[16], part), 71), part)
    values = scatter_about(part_keys[2], (SEQUENCE_LENGTH, HEADS, HD), 1.0, 6.0, ((0, 32), (1, 4)))
    forget_cum = draw_forget_cum(jax.random.fold_in(jax.random.fold_in(streams_of[16], part), 71), part)
    query_gain = draw_query_gain(jax.random.fold_in(streams_of[16], 71), part)
    key_gain = draw_key_gain(jax.random.fold_in(streams_of[16], 71), part)
    tokens = scatter_about(part_keys[6], (TOKENS_B, D), 1.0, 6.0, ((0, 128),))
    norm_gain = jnp.clip(1.0 + 0.18 * jax.random.normal(streams_of[7], (D,), jnp.float32), 0.1, 1.9)
    routes_keys = jax.random.split(jax.random.fold_in(part_keys[8], 1), TOKENS_B // TOK_B)
    routes_turns = jax.random.permutation(jax.random.fold_in(part_keys[8], 3), TOKENS_B // TOK_B)
    routes = jax.vmap(lambda own, number: deal_out(jax.random.fold_in(part_keys[8], 2), own, number, TOK_B, EXPERTS, TOP_K, CAP, 0))(routes_keys, routes_turns).reshape((TOKENS_B, TOP_K))
    route_weights = jnp.clip(0.3 + 0.90000004 * jax.random.uniform(part_keys[9], (TOKENS_B, TOP_K), jnp.float32) ** block_levels(part_keys[9], (TOKENS_B, TOP_K), ((0, 128),), -0.2, 0.2), 0.3, 1.2)
    expert_gate = scatter_about(streams_of[10], (EXPERTS, D, EF), D ** -0.5, 0.09375, ((0, 128),))
    expert_up = scatter_about(streams_of[11], (EXPERTS, D, EF), D ** -0.5, 0.09375, ((0, 128),))
    expert_down = scatter_about(streams_of[12], (EXPERTS, EF, D), EF ** -0.5, 0.3125, ((0, 128),))
    shared_gate = scatter_about(streams_of[13], (D, SF), D ** -0.5, 0.09375, ((1, 4),))
    shared_up = scatter_about(streams_of[14], (D, SF), D ** -0.5, 0.09375, ((1, 4),))
    shared_down = scatter_about(streams_of[15], (SF, D), SF ** -0.5, 0.4375, ((0, 4),))
    return {"queries": queries, "key_vectors": key_vectors, "values": values, "forget_cum": forget_cum, "query_gain": query_gain, "key_gain": key_gain, "tokens": tokens, "norm_gain": norm_gain, "routes": routes, "route_weights": route_weights, "expert_gate": expert_gate, "expert_up": expert_up, "expert_down": expert_down, "shared_gate": shared_gate, "shared_up": shared_up, "shared_down": shared_down}


def rms_rows(row_values, gain_vector):
    widened = row_values.astype(jnp.float32)
    inverse = lax.rsqrt(lax.optimization_barrier(jnp.mean(widened * widened, axis=-1, keepdims=True)) + 1e-06)
    return (widened * inverse * gain_vector.astype(jnp.float32)).astype(jnp.bfloat16)

def attention(queries, key_vectors, values, forget_cum, query_gain, key_gain):
    query_norm = lax.optimization_barrier(rms_rows(queries, query_gain)).astype(jnp.float32)
    key_norm = lax.optimization_barrier(rms_rows(key_vectors, key_gain)).astype(jnp.float32)
    value_wide = values.astype(jnp.float32)
    length = queries.shape[0]
    block_rows = 512 if length % 512 == 0 else length
    scale_factor = queries.shape[2] ** (-0.5)
    outputs = []
    for first_row in range(0, length, block_rows):
        stop_row = first_row + block_rows
        scores = jnp.einsum('qhd,khd->hqk', query_norm[first_row:stop_row], key_norm[:stop_row]) * scale_factor
        scores = scores + forget_cum[first_row:stop_row].T[:, :, None] - forget_cum[:stop_row].T[:, None, :]
        allowed = (jnp.arange(stop_row)[None, :] <= jnp.arange(first_row, stop_row)[:, None])[None]
        scores = jnp.where(allowed, scores, -jnp.inf)
        row_max = lax.optimization_barrier(jnp.max(scores, axis=2, keepdims=True))
        weights = jnp.exp(scores - row_max)
        denominator = lax.optimization_barrier(jnp.sum(weights, axis=2))
        probabilities = lax.optimization_barrier(weights.astype(jnp.bfloat16)).astype(jnp.float32)
        mixed_rows = jnp.einsum('hqk,khd->hqd', probabilities, value_wide[:stop_row]) / denominator[:, :, None]
        outputs.append(mixed_rows.transpose(1, 0, 2))
    return jnp.concatenate(outputs, axis=0).astype(jnp.bfloat16)

def mixture(tokens, norm_gain, routes, route_weights, expert_gate, expert_up, expert_down, shared_gate, shared_up, shared_down):
    normed = rms_rows(tokens, norm_gain)
    row_total = tokens.shape[0]
    shared_hidden = (jax.nn.silu(jnp.dot(normed, shared_gate, preferred_element_type=jnp.float32)) * jnp.dot(normed, shared_up, preferred_element_type=jnp.float32)).astype(jnp.bfloat16)
    part_width = shared_down.shape[0] // N_TP
    shared_sum = jnp.zeros((row_total, tokens.shape[1]), jnp.float32)
    for block_index in range(N_TP):
        low = block_index * part_width
        partial_value = jnp.dot(shared_hidden[:, low:low + part_width], shared_down[low:low + part_width], preferred_element_type=jnp.float32)
        shared_sum = shared_sum + lax.optimization_barrier(partial_value.astype(jnp.bfloat16)).astype(jnp.float32)
    shared_out = shared_sum.astype(jnp.bfloat16)
    block_count = N_EP * N_TP
    per_block = routes.reshape(block_count, -1)
    choices_per = per_block.shape[1]
    token_index = (jnp.arange(block_count)[:, None] * (choices_per // TOP_K) + jnp.arange(choices_per)[None, :] // TOP_K).astype(jnp.int32)
    weight_table = route_weights.reshape(block_count, -1)
    one_hot = (per_block[:, :, None] == jnp.arange(EXPERTS)[None, None, :]).astype(jnp.int32)
    slot_rank = lax.optimization_barrier(jnp.sum((jnp.cumsum(one_hot, axis=1) - one_hot) * one_hot, axis=2))

    def one_expert(running_sum, expert_index):
        chosen = per_block == expert_index
        placed = chosen[:, :, None] & (slot_rank[:, :, None] == jnp.arange(CAP)[None, None, :])
        row_ids = lax.optimization_barrier(jnp.sum(jnp.where(placed, token_index[:, :, None], 0), axis=1)).reshape(-1).astype(jnp.int32)
        slot_weight = lax.optimization_barrier(jnp.sum(jnp.where(placed, weight_table[:, :, None], 0.0), axis=1)).reshape(-1)
        picked = normed[row_ids]
        gate_values = jnp.dot(picked, expert_gate[expert_index], preferred_element_type=jnp.float32)
        upward = jnp.dot(picked, expert_up[expert_index], preferred_element_type=jnp.float32)
        hidden = (jax.nn.silu(gate_values) * upward).astype(jnp.bfloat16)
        produced = jnp.dot(hidden, expert_down[expert_index], preferred_element_type=jnp.float32).astype(jnp.bfloat16)
        produced = lax.optimization_barrier(produced).astype(jnp.float32)
        return (running_sum.at[row_ids].add(slot_weight[:, None] * produced), None)
    routed, _ = lax.scan(one_expert, jnp.zeros((row_total, tokens.shape[1]), jnp.float32), jnp.arange(EXPERTS).astype(jnp.int32))
    return (shared_out.astype(jnp.float32) + routed).astype(jnp.bfloat16)

def reference(queries, key_vectors, values, forget_cum, query_gain, key_gain, tokens, norm_gain, routes, route_weights, expert_gate, expert_up, expert_down, shared_gate, shared_up, shared_down):
    attended = attention(queries, key_vectors, values, forget_cum, query_gain, key_gain)
    routed_output = mixture(tokens, norm_gain, routes, route_weights, expert_gate, expert_up, expert_down, shared_gate, shared_up, shared_down)
    return (attended, routed_output)
```

```python
import functools

import jax
import jax.numpy as jnp
from jax import lax
from jax.experimental import pallas as pl
from jax.experimental.pallas import tpu as pltpu
from jax.sharding import PartitionSpec as P

MESH = pl.DeviceIdType.MESH
CORES = 2
CHUNKS = 4
BF = jnp.bfloat16
F32 = jnp.float32


def dot_nn(a, b):
    return lax.dot_general(a, b, (((1,), (0,)), ((), ())), preferred_element_type=F32)


def dot_nt(a, b):
    return lax.dot_general(a, b, (((1,), (1,)), ((), ())), preferred_element_type=F32)


def rms(values, gain):
    wide = values.astype(F32)
    inverse = lax.rsqrt(jnp.mean(wide * wide, axis=-1, keepdims=True) + 1e-06)
    return (wide * inverse * gain).astype(BF)


def kernel(
    nz,
    nx,
    q_in,
    k_in,
    v_in,
    fc_in,
    qgain_in,
    kgain_in,
    tokens_in,
    ngain_in,
    routes_in,
    weights_in,
    sgate_in,
    sup_in,
    sdown_in,
    gate_hbm,
    up_hbm,
    down_hbm,
    att_out,
    rout_out,
    gate_v,
    up_v,
    down_v,
    normed_v,
    outgoing,
    zbuf,
    xout,
    xbuf,
    yout,
    ybuf,
    zout,
    rbuf,
    sel_v,
    mix_v,
    acc_g,
    acc_u,
    hidden_v,
    shbuf,
    sh_v,
    fcbuf,
    s1,
    hbuf,
    kvbuf,
    qn_v,
    kvown,
    scores_v,
    o_v,
    obuf,
    wsem,
    osem,
    send_z,
    recv_z,
    send_x,
    recv_x,
    send_rx,
    recv_rx,
    send_rz,
    recv_rz,
    send_m,
    recv_m,
):
    n_plane = CORES * nx
    rows = tokens_in.shape[0]
    width = tokens_in.shape[1]
    cw = width // CHUNKS
    slots = nz * n_plane * 2
    quarter = rows // nx
    hd = qgain_in.shape[1]
    heads = q_in.shape[1] // hd
    length = nz * CORES * rows

    ep = lax.axis_index("ep")
    x = lax.axis_index("tp")
    z = ep // CORES
    c = ep % CORES
    q = c * nx + x

    def dev(z_, c_, x_):
        return {"ep": z_ * CORES + c_, "tp": x_}

    def plane_dev(q_):
        return dev(z, q_ // nx, q_ % nx)

    far = []
    for d in range(nz // 2, 0, -1):
        far.append(d)
        if 2 * d != nz:
            far.append(nz - d)

    def remote(src, dst, s_sem, r_sem, device):
        return pltpu.make_async_remote_copy(
            src_ref=src, dst_ref=dst, send_sem=s_sem, recv_sem=r_sem, device_id=device, device_id_type=MESH
        )

    def done(ref, s_sem, r_sem, sent):
        copy = remote(ref, ref, s_sem, r_sem, dev(z, c, x))
        if sent:
            copy.wait_send()
        else:
            copy.wait_recv()

    weight_copies = [
        pltpu.make_async_copy(gate_hbm.at[0], gate_v, wsem.at[0]),
        pltpu.make_async_copy(up_hbm.at[0], up_v, wsem.at[1]),
    ] + [
        pltpu.make_async_copy(down_hbm.at[0, :, pl.ds(j * cw, cw)], down_v.at[j], wsem.at[2 + j])
        for j in range(CHUNKS)
    ]
    for copy in weight_copies:
        copy.start()

    barrier = pltpu.get_barrier_semaphore()
    for d in far:
        pl.semaphore_signal(barrier, inc=1, device_id=dev((z + d) % nz, c, x), device_id_type=MESH)
    for d in range(1, n_plane):
        pl.semaphore_signal(barrier, inc=1, device_id=plane_dev((q + d) % n_plane), device_id_type=MESH)
    pl.semaphore_wait(barrier, len(far) + n_plane - 1)

    for i, ref in enumerate((q_in, k_in, v_in)):
        for d in range(1, nx):
            x_ = (x + d) % nx
            remote(
                ref.at[pl.ds(x_ * quarter, quarter)], s1.at[i, x], send_m.at[0], recv_m.at[0], dev(z, c, x_)
            ).start()
    for d in range(1, nx):
        remote(fc_in, fcbuf.at[x], send_m.at[1], recv_m.at[1], dev(z, c, (x + d) % nx)).start()
    for i, ref in enumerate((q_in, k_in, v_in)):
        s1[i, x] = ref[pl.ds(pl.multiple_of(x * quarter, quarter), quarter), :]
    fcbuf[x] = fc_in[...]

    slot = lax.broadcasted_iota(jnp.int32, (slots, rows), 0)
    expert = (slot // (2 * n_plane)) * n_plane + slot % n_plane
    copy_of = (slot // n_plane) % 2
    first = (routes_in[0:1, :] == expert).astype(F32)
    second = (routes_in[1:2, :] == expert).astype(F32)
    named = first + second
    earlier = (
        lax.broadcasted_iota(jnp.int32, (rows, rows), 0) < lax.broadcasted_iota(jnp.int32, (rows, rows), 1)
    ).astype(BF)
    rank = dot_nn(named.astype(BF), earlier)
    mine = jnp.where(rank == copy_of.astype(F32), 1.0, 0.0)
    sel_v[...] = (named * mine).astype(BF)
    mix = (mine * (first * weights_in[0:1, :] + second * weights_in[1:2, :])).T
    high = mix.astype(BF)
    left = mix - high.astype(F32)
    middle = left.astype(BF)
    mix_v[0] = high
    mix_v[1] = middle
    mix_v[2] = (left - middle.astype(F32)).astype(BF)

    total = jnp.zeros((rows, 1), F32)
    for j in range(CHUNKS):
        part = tokens_in[:, j * cw : (j + 1) * cw].astype(F32)
        total = total + jnp.sum(part * part, axis=-1, keepdims=True)
    inverse = lax.rsqrt(total / width + 1e-06)

    def dispatch(j, carry):
        at = pl.ds(pl.multiple_of(j * cw, cw), cw)
        part = (tokens_in[:, at].astype(F32) * inverse * ngain_in[:, at]).astype(BF)
        normed_v[j] = part
        picked = dot_nn(sel_v[...], part).astype(BF)
        outgoing[j] = picked.reshape(nz, 2 * n_plane, cw)
        for d in far:
            z_ = (z + d) % nz
            remote(outgoing.at[j, z_], zbuf.at[j, z], send_z.at[j], recv_z.at[j], dev(z_, c, x)).start()
        zbuf[j, z] = outgoing[j, z]
        return carry

    lax.fori_loop(0, CHUNKS, dispatch, 0)

    done(s1.at[:, pl.ds(0, nx - 1)], send_m.at[0], recv_m.at[0], False)
    for d in far:
        z_ = (z + d) % nz
        lanes = pl.ds(pl.multiple_of((z_ % heads) * hd, hd), hd)
        remote(
            s1.at[:, z_ // heads, :, lanes], hbuf.at[:, z], send_m.at[2], recv_m.at[2], dev(z_, c, x)
        ).start()
    for i in range(3):
        hbuf[i, z] = s1[i, z // heads, :, pl.ds(pl.multiple_of((z % heads) * hd, hd), hd)]

    for i, ref in enumerate((sgate_in, sup_in, sdown_in)):
        for d in range(1, nx):
            remote(ref, shbuf.at[x, i], send_m.at[3], recv_m.at[3], dev(z, c, (x + d) % nx)).start()
        shbuf[x, i] = ref[...]
    done(shbuf.at[pl.ds(0, nx - 1)], send_m.at[3], recv_m.at[3], False)

    shared_rows = [[None, None] for _ in range(nx)]
    hiddens = []
    for n in range(nx):
        gate_sum = jnp.zeros((rows, sgate_in.shape[0]), F32)
        up_sum = jnp.zeros((rows, sgate_in.shape[0]), F32)
        for j in range(CHUNKS):
            gate_sum = gate_sum + dot_nt(normed_v[j], shbuf[n, 0, :, j * cw : (j + 1) * cw])
            up_sum = up_sum + dot_nt(normed_v[j], shbuf[n, 1, :, j * cw : (j + 1) * cw])
        hiddens.append((gate_sum / (1.0 + jnp.exp(-gate_sum)) * up_sum).astype(BF))

    def shared_down(j, carry):
        at = pl.ds(pl.multiple_of(j * cw, cw), cw)
        out = jnp.zeros((rows, cw), F32)
        for n in range(nx):
            out = out + dot_nn(hiddens[n], shbuf[n, 2, :, at]).astype(BF).astype(F32)
        sh_v[j] = out.astype(BF)
        return carry

    lax.fori_loop(0, CHUNKS, shared_down, 0)

    to_row = lax.broadcasted_iota(jnp.int32, (slots, slots), 0)
    from_row = lax.broadcasted_iota(jnp.int32, (slots, slots), 1)
    span = 2 * nz
    by_device = (
        from_row == ((to_row % span) // 2) * (2 * n_plane) + (to_row % 2) * n_plane + to_row // span
    ).astype(BF)
    by_plane = (
        to_row == ((from_row % span) // 2) * (2 * n_plane) + (from_row % 2) * n_plane + from_row // span
    ).astype(BF)

    weight_copies[0].wait()
    weight_copies[1].wait()
    acc_g[...] = jnp.zeros_like(acc_g)
    acc_u[...] = jnp.zeros_like(acc_u)

    def spread(j, carry):
        done(zbuf.at[j, pl.ds(0, nz - 1)], send_z.at[j], recv_z.at[j], False)
        moved = dot_nn(by_device, zbuf[j].reshape(slots, cw)).astype(BF)
        xout[j] = moved.reshape(n_plane, span, cw)
        for d in range(1, n_plane):
            q_ = (q + d) % n_plane
            remote(xout.at[j, q_], xbuf.at[j, q], send_x.at[j], recv_x.at[j], plane_dev(q_)).start()
        xbuf[j, q] = xout[j, q]
        done(xbuf.at[j, pl.ds(0, n_plane - 1)], send_x.at[j], recv_x.at[j], False)
        arrived = xbuf[j].reshape(slots, cw)
        at = pl.ds(pl.multiple_of(j * cw, cw), cw)
        acc_g[...] += dot_nn(arrived, gate_v[at, :])
        acc_u[...] += dot_nn(arrived, up_v[at, :])
        return carry

    lax.fori_loop(0, CHUNKS, spread, 0)

    for copy in weight_copies[2:]:
        copy.wait()
    gates = acc_g[...]
    hidden_v[...] = (gates / (1.0 + jnp.exp(-gates)) * acc_u[...]).astype(BF)

    def produce(j, carry):
        made = dot_nn(hidden_v[...], down_v[j]).astype(BF)
        yout[j] = made.reshape(n_plane, span, cw)
        for d in range(1, n_plane):
            q_ = (q + d) % n_plane
            remote(yout.at[j, q_], ybuf.at[j, q], send_rx.at[j], recv_rx.at[j], plane_dev(q_)).start()
        ybuf[j, q] = yout[j, q]
        return carry

    def give_back(j, carry):
        done(ybuf.at[j, pl.ds(0, n_plane - 1)], send_rx.at[j], recv_rx.at[j], False)
        moved = dot_nn(by_plane, ybuf[j].reshape(slots, cw)).astype(BF)
        zout[j] = moved.reshape(nz, 2 * n_plane, cw)
        for d in far:
            z_ = (z + d) % nz
            remote(zout.at[j, z_], rbuf.at[j, z], send_rz.at[j], recv_rz.at[j], dev(z_, c, x)).start()
        rbuf[j, z] = zout[j, z]
        return carry

    lax.fori_loop(0, CHUNKS, produce, 0)
    lax.fori_loop(0, CHUNKS // 2, give_back, 0)

    done(hbuf.at[:, pl.ds(0, nz - 1)], send_m.at[2], recv_m.at[2], False)
    share = nz * quarter
    qn_v[...] = rms(hbuf[0].reshape(share, hd), qgain_in[...])
    kvown[0] = rms(hbuf[1].reshape(share, hd), kgain_in[...]).reshape(nz, quarter, hd)
    kvown[1] = hbuf[2]
    for d in range(1, n_plane):
        q_ = (q + d) % n_plane
        remote(kvown, kvbuf.at[:, :, c, x], send_m.at[4], recv_m.at[4], plane_dev(q_)).start()
    for i in range(2):
        kvbuf[i, :, c, x] = kvown[i]
    others = kvbuf.at[:, pl.ds(0, nz * (n_plane - 1) // n_plane)]
    done(fcbuf.at[pl.ds(0, nx - 1)], send_m.at[1], recv_m.at[1], False)
    bias = fcbuf[z // heads, pl.ds(z % heads, 1), :]
    scale = hd ** (-0.5)
    done(others, send_m.at[4], recv_m.at[4], False)
    key_at = lax.broadcasted_iota(jnp.int32, (rows, length), 1)
    block = lax.broadcasted_iota(jnp.int32, (rows, 1), 0)

    def attend(b, carry):
        mine_at = block + b * rows
        query_at = ((mine_at // quarter) * CORES + c) * rows + x * quarter + mine_at % quarter
        keys = kvbuf[0].reshape(length, hd)
        scores = dot_nt(qn_v[pl.ds(pl.multiple_of(b * rows, rows), rows), :], keys) * scale - bias
        scores = jnp.where(key_at <= query_at, scores, -1e30)
        scores_v[...] = scores
        best = jnp.max(scores, axis=1, keepdims=True)
        weights = jnp.exp(scores_v[...] - best)
        below = jnp.sum(weights, axis=1, keepdims=True)
        mixed = dot_nn(weights.astype(BF), kvbuf[1].reshape(length, hd)) / below
        per = rows // quarter
        o_v[pl.ds(b * per, per)] = mixed.astype(BF).reshape(per, quarter, hd)
        return carry

    lax.fori_loop(0, share // rows, attend, 0)
    for d in far:
        z_ = (z + d) % nz
        remote(o_v.at[z_], obuf.at[z], send_m.at[5], recv_m.at[5], dev(z_, c, x)).start()
    obuf[z] = o_v[z]

    lax.fori_loop(CHUNKS // 2, CHUNKS, give_back, 0)

    def combine(j, carry):
        done(rbuf.at[j, pl.ds(0, nz - 1)], send_rz.at[j], recv_rz.at[j], False)
        got = rbuf[j].reshape(slots, cw)
        routed = dot_nn(mix_v[0], got) + dot_nn(mix_v[1], got) + dot_nn(mix_v[2], got)
        at = pl.ds(pl.multiple_of(j * cw, cw), cw)
        rout_out[:, at] = (sh_v[j].astype(F32) + routed).astype(BF)
        return carry

    lax.fori_loop(0, CHUNKS // 2, combine, 0)

    done(obuf.at[pl.ds(0, nz - 1)], send_m.at[5], recv_m.at[5], False)
    here = pl.ds(pl.multiple_of(x * quarter, quarter), quarter)
    for d in range(1, nx):
        x_ = (x + d) % nx
        for h in range(heads):
            remote(
                obuf.at[x_ * heads + h],
                att_out.at[here, pl.ds(h * hd, hd)],
                send_m.at[6],
                recv_m.at[6],
                dev(z, c, x_),
            ).start()
    for h in range(heads):
        att_out[here, h * hd : (h + 1) * hd] = obuf[x * heads + h]

    lax.fori_loop(CHUNKS // 2, CHUNKS, combine, 0)

    done(att_out.at[pl.ds(0, (nx - 1) * quarter)], send_m.at[6], recv_m.at[6], False)

    def drain(j, carry):
        done(zbuf.at[j, pl.ds(0, nz - 1)], send_z.at[j], recv_z.at[j], True)
        done(xbuf.at[j, pl.ds(0, n_plane - 1)], send_x.at[j], recv_x.at[j], True)
        done(ybuf.at[j, pl.ds(0, n_plane - 1)], send_rx.at[j], recv_rx.at[j], True)
        done(rbuf.at[j, pl.ds(0, nz - 1)], send_rz.at[j], recv_rz.at[j], True)
        return carry

    lax.fori_loop(0, CHUNKS, drain, 0)
    done(s1.at[:, pl.ds(0, nx - 1)], send_m.at[0], recv_m.at[0], True)
    done(fcbuf.at[pl.ds(0, nx - 1)], send_m.at[1], recv_m.at[1], True)
    done(hbuf.at[:, pl.ds(0, nz - 1)], send_m.at[2], recv_m.at[2], True)
    done(shbuf.at[pl.ds(0, nx - 1)], send_m.at[3], recv_m.at[3], True)
    done(others, send_m.at[4], recv_m.at[4], True)
    done(obuf.at[pl.ds(0, nz - 1)], send_m.at[5], recv_m.at[5], True)
    done(att_out.at[pl.ds(0, (nx - 1) * quarter)], send_m.at[6], recv_m.at[6], True)


def solution(mesh):
    nx = mesh.shape["tp"]
    nz = mesh.shape["ep"] // CORES

    def local(
        queries,
        key_vectors,
        values,
        forget_cum,
        query_gain,
        key_gain,
        tokens,
        norm_gain,
        routes,
        route_weights,
        expert_gate,
        expert_up,
        expert_down,
        shared_gate,
        shared_up,
        shared_down,
    ):
        rows, heads, hd = queries.shape
        width = tokens.shape[1]
        hidden = expert_gate.shape[2]
        part = shared_down.shape[0]
        length = forget_cum.shape[0]
        n_plane = CORES * nx
        slots = nz * n_plane * 2
        cw = width // CHUNKS
        quarter = rows // nx
        share = nz * quarter
        vm = pl.BlockSpec(memory_space=pltpu.VMEM)
        hbm = pl.BlockSpec(memory_space=pl.ANY)
        V = pltpu.VMEM
        by_plane = V((CHUNKS, nz, 2 * n_plane, cw), BF)
        by_device = V((CHUNKS, n_plane, 2 * nz, cw), BF)
        dma = pltpu.SemaphoreType.DMA
        att, out = pl.pallas_call(
            functools.partial(kernel, nz, nx),
            out_shape=(
                jax.ShapeDtypeStruct((rows, heads * hd), BF),
                jax.ShapeDtypeStruct((rows, width), BF),
            ),
            in_specs=[vm] * 13 + [hbm] * 3,
            out_specs=(vm, vm),
            scratch_shapes=[
                V((width, hidden), BF),
                V((width, hidden), BF),
                V((CHUNKS, hidden, cw), BF),
                V((CHUNKS, rows, cw), BF),
                by_plane,
                by_plane,
                by_device,
                by_device,
                by_device,
                by_device,
                by_plane,
                by_plane,
                V((slots, rows), BF),
                V((3, rows, slots), BF),
                V((slots, hidden), F32),
                V((slots, hidden), F32),
                V((slots, hidden), BF),
                V((nx, 3, part, width), BF),
                V((CHUNKS, rows, cw), BF),
                V((nx, heads, length), F32),
                V((3, nx, quarter, heads * hd), BF),
                V((3, nz, quarter, hd), BF),
                V((2, nz, CORES, nx, quarter, hd), BF),
                V((share, hd), BF),
                V((2, nz, quarter, hd), BF),
                V((rows, length), F32),
                V((nz, quarter, hd), BF),
                V((nz, quarter, hd), BF),
                dma((2 + CHUNKS,)),
                dma((1,)),
            ]
            + [dma((CHUNKS,))] * 8
            + [dma((7,))] * 2,
            compiler_params=pltpu.CompilerParams(
                collective_id=0, has_side_effects=True, vmem_limit_bytes=63 * 1024 * 1024
            ),
        )(
            queries.reshape(rows, heads * hd),
            key_vectors.reshape(rows, heads * hd),
            values.reshape(rows, heads * hd),
            forget_cum.T,
            query_gain.reshape(1, hd),
            key_gain.reshape(1, hd),
            tokens,
            norm_gain.reshape(1, width),
            routes.T,
            route_weights.T,
            shared_gate.T,
            shared_up.T,
            shared_down,
            expert_gate,
            expert_up,
            expert_down,
        )
        return att.reshape(rows, heads, hd), out

    placed = (
        P(("grp", "ep"), "tp", None),
        P(("grp", "ep"), "tp", None),
        P(("grp", "ep"), "tp", None),
        P("grp", "tp"),
        P(),
        P(),
        P(("grp", "ep", "tp"), None),
        P(),
        P(("grp", "ep", "tp"), None),
        P(("grp", "ep", "tp"), None),
        P(("ep", "tp"), None, None),
        P(("ep", "tp"), None, None),
        P(("ep", "tp"), None, None),
        P(None, "tp"),
        P(None, "tp"),
        P("tp", None),
    )
    return jax.shard_map(
        local,
        mesh=mesh,
        in_specs=placed,
        out_specs=(P(("grp", "ep"), "tp", None), P(("grp", "ep", "tp"), None)),
        check_vma=False,
    )
```

```python
import functools

import jax
import jax.numpy as jnp
from jax import lax
from jax.experimental import pallas as pl
from jax.experimental.pallas import tpu as pltpu
from jax.sharding import PartitionSpec as P

MESH = pl.DeviceIdType.MESH
CORES = 2
CHUNKS = 4
VLIM = 63
BF = jnp.bfloat16
F32 = jnp.float32


def columns(j, size):
    return pl.ds(j * size if isinstance(j, int) else pl.multiple_of(j * size, size), size)


def steps(first, last, body):
    if last - first == 1:
        body(first, 0)
    else:
        lax.fori_loop(first, last, body, 0)


def dot_nn(a, b):
    return lax.dot_general(a, b, (((1,), (0,)), ((), ())), preferred_element_type=F32)


def dot_nt(a, b):
    return lax.dot_general(a, b, (((1,), (1,)), ((), ())), preferred_element_type=F32)


def rms(values, gain):
    wide = values.astype(F32)
    inverse = lax.rsqrt(jnp.mean(wide * wide, axis=-1, keepdims=True) + 1e-06)
    return (wide * inverse * gain).astype(BF)


def kernel(
    nz,
    nx,
    q_hbm,
    k_hbm,
    v_hbm,
    fc_hbm,
    qgain_hbm,
    kgain_hbm,
    tokens_hbm,
    ngain_hbm,
    routes_hbm,
    weights_hbm,
    sgate_hbm,
    sup_hbm,
    sdown_hbm,
    gate_hbm,
    up_hbm,
    down_hbm,
    att_out,
    rout_out,
    made_v,
    outsem,
    gate_v,
    up_v,
    down_v,
    normed_v,
    outgoing,
    zbuf,
    xout,
    xbuf,
    yout,
    ybuf,
    zout,
    rbuf,
    sel_v,
    mix_v,
    acc_g,
    acc_u,
    hidden_v,
    shbuf,
    sh_v,
    fcbuf,
    fc_in,
    qgain_in,
    kgain_in,
    ngain_in,
    routes_in,
    weights_in,
    tokens_in,
    qkv_in,
    s1raw,
    s1,
    hbuf,
    kvbuf,
    qn_v,
    kvown,
    scores_v,
    o_v,
    obuf,
    fbuf,
    wsem,
    osem,
    send_z,
    recv_z,
    send_x,
    recv_x,
    send_rx,
    recv_rx,
    send_rz,
    recv_rz,
    send_m,
    recv_m,
):
    n_plane = CORES * nx
    rows = tokens_hbm.shape[0]
    width = tokens_hbm.shape[1]
    cw = width // CHUNKS
    slots = nz * n_plane * 2
    quarter = rows // nx
    hd = qgain_hbm.shape[1]
    heads = q_hbm.shape[0] // rows
    length = nz * CORES * rows

    ep = lax.axis_index("ep")
    x = lax.axis_index("tp")
    z = ep // CORES
    c = ep % CORES
    q = c * nx + x

    def dev(z_, c_, x_):
        return {"ep": z_ * CORES + c_, "tp": x_}

    def plane_dev(q_):
        return dev(z, q_ // nx, q_ % nx)

    far = []
    for d in range(nz // 2, 0, -1):
        far.append(d)
        if 2 * d != nz:
            far.append(nz - d)

    def remote(src, dst, s_sem, r_sem, device):
        return pltpu.make_async_remote_copy(
            src_ref=src, dst_ref=dst, send_sem=s_sem, recv_sem=r_sem, device_id=device, device_id_type=MESH
        )

    def done(ref, s_sem, r_sem, sent):
        copy = remote(ref, ref, s_sem, r_sem, dev(z, c, x))
        if sent:
            copy.wait_send()
        else:
            copy.wait_recv()

    barrier = pltpu.get_barrier_semaphore()
    for d in far:
        pl.semaphore_signal(barrier, inc=1, device_id=dev((z + d) % nz, c, x), device_id_type=MESH)
    for d in range(1, n_plane):
        pl.semaphore_signal(barrier, inc=1, device_id=plane_dev((q + d) % n_plane), device_id_type=MESH)

    token_copy = pltpu.make_async_copy(tokens_hbm, tokens_in, osem.at[0])
    token_copy.start()
    own_copies = [
        pltpu.make_async_copy(ref, qkv_in.at[i], osem.at[1 + i]) for i, ref in enumerate((q_hbm, k_hbm, v_hbm))
    ] + [
        pltpu.make_async_copy(ref, shbuf.at[x, i], osem.at[4 + i])
        for i, ref in enumerate((sgate_hbm, sup_hbm, sdown_hbm))
    ]
    small_copies = [
        pltpu.make_async_copy(src, dst, osem.at[7 + i])
        for i, (src, dst) in enumerate(
            (
                (routes_hbm, routes_in),
                (weights_hbm, weights_in),
                (ngain_hbm, ngain_in),
                (qgain_hbm, qgain_in),
                (kgain_hbm, kgain_in),
                (fc_hbm, fc_in),
            )
        )
    ]
    for copy in small_copies + own_copies:
        copy.start()
    weight_copies = [
        pltpu.make_async_copy(gate_hbm.at[0], gate_v, wsem.at[0]),
        pltpu.make_async_copy(up_hbm.at[0], up_v, wsem.at[1]),
    ] + [
        pltpu.make_async_copy(down_hbm.at[0, :, pl.ds(j * cw, cw)], down_v.at[j], wsem.at[2 + j])
        for j in range(CHUNKS)
    ]
    for copy in weight_copies:
        copy.start()

    for copy in small_copies:
        copy.wait()

    slot = lax.broadcasted_iota(jnp.int32, (slots, rows), 0)
    expert = (slot // (2 * n_plane)) * n_plane + slot % n_plane
    copy_of = (slot // n_plane) % 2
    first = (routes_in[0:1, :] == expert).astype(F32)
    second = (routes_in[1:2, :] == expert).astype(F32)
    named = first + second
    earlier = (
        lax.broadcasted_iota(jnp.int32, (rows, rows), 0) < lax.broadcasted_iota(jnp.int32, (rows, rows), 1)
    ).astype(BF)
    rank = dot_nn(named.astype(BF), earlier)
    mine = jnp.where(rank == copy_of.astype(F32), 1.0, 0.0)
    sel_v[...] = (named * mine).astype(BF)
    mix = (mine * (first * weights_in[0:1, :] + second * weights_in[1:2, :])).T
    high = mix.astype(BF)
    left = mix - high.astype(F32)
    middle = left.astype(BF)
    mix_v[0] = high
    mix_v[1] = middle
    mix_v[2] = (left - middle.astype(F32)).astype(BF)

    token_copy.wait()
    total = jnp.zeros((rows, 1), F32)
    for j in range(CHUNKS):
        part = tokens_in[:, j * cw : (j + 1) * cw].astype(F32)
        total = total + jnp.sum(part * part, axis=-1, keepdims=True)
    inverse = lax.rsqrt(total / width + 1e-06)

    pl.semaphore_wait(barrier, len(far) + n_plane - 1)

    def dispatch(j, carry):
        at = columns(j, cw)
        part = (tokens_in[:, at].astype(F32) * inverse * ngain_in[:, at]).astype(BF)
        normed_v[j] = part
        picked = dot_nn(sel_v[...], part).astype(BF)
        outgoing[j] = picked.reshape(nz, 2 * n_plane, cw)
        for d in far:
            z_ = (z + d) % nz
            remote(outgoing.at[j, z_], zbuf.at[j, z], send_z.at[j], recv_z.at[j], dev(z_, c, x)).start()
        zbuf[j, z] = outgoing[j, z]
        return carry

    steps(0, 1, dispatch)

    block_rows = quarter * heads
    for copy in own_copies[:3]:
        copy.wait()
    for d in range(1, nx):
        x_ = (x + d) % nx
        remote(
            qkv_in.at[:, pl.ds(pl.multiple_of(x_ * block_rows, block_rows), block_rows)],
            s1raw.at[x],
            send_m.at[0],
            recv_m.at[0],
            dev(z, c, x_),
        ).start()
        remote(fc_in, fcbuf.at[x], send_m.at[1], recv_m.at[1], dev(z, c, x_)).start()
    s1raw[x] = qkv_in[:, pl.ds(pl.multiple_of(x * block_rows, block_rows), block_rows)]
    fcbuf[x] = fc_in[...]

    steps(1, CHUNKS, dispatch)

    by_head_to = lax.broadcasted_iota(jnp.int32, (block_rows, block_rows), 0)
    by_head_from = lax.broadcasted_iota(jnp.int32, (block_rows, block_rows), 1)
    by_head = (by_head_from == (by_head_to % quarter) * heads + by_head_to // quarter).astype(BF)
    by_position = (by_head_to == (by_head_from % quarter) * heads + by_head_from // quarter).astype(BF)
    done(s1raw.at[pl.ds(0, nx - 1)], send_m.at[0], recv_m.at[0], False)
    for x_ in range(nx):
        for i in range(3):
            s1[i, x_ * heads : (x_ + 1) * heads] = (
                dot_nn(by_head, s1raw[x_, i]).astype(BF).reshape(heads, quarter, hd)
            )
    for d in far:
        z_ = (z + d) % nz
        remote(s1.at[:, z_], hbuf.at[:, z], send_m.at[2], recv_m.at[2], dev(z_, c, x)).start()
    for i in range(3):
        hbuf[i, z] = s1[i, z]

    for copy in own_copies[3:]:
        copy.wait()
    for d in range(1, nx):
        remote(shbuf.at[x], shbuf.at[x], send_m.at[3], recv_m.at[3], dev(z, c, (x + d) % nx)).start()
    done(shbuf.at[pl.ds(0, nx - 1)], send_m.at[3], recv_m.at[3], False)

    hiddens = []
    for n in range(nx):
        gate_sum = jnp.zeros((rows, sgate_hbm.shape[0]), F32)
        up_sum = jnp.zeros((rows, sgate_hbm.shape[0]), F32)
        for j in range(CHUNKS):
            gate_sum = gate_sum + dot_nt(normed_v[j], shbuf[n, 0, :, j * cw : (j + 1) * cw])
            up_sum = up_sum + dot_nt(normed_v[j], shbuf[n, 1, :, j * cw : (j + 1) * cw])
        hiddens.append((gate_sum / (1.0 + jnp.exp(-gate_sum)) * up_sum).astype(BF))

    def shared_down(j, carry):
        at = columns(j, cw)
        out = jnp.zeros((rows, cw), F32)
        for n in range(nx):
            out = out + dot_nn(hiddens[n], shbuf[n, 2, :, at]).astype(BF).astype(F32)
        sh_v[j] = out.astype(BF)
        return carry

    steps(0, CHUNKS, shared_down)

    to_row = lax.broadcasted_iota(jnp.int32, (slots, slots), 0)
    from_row = lax.broadcasted_iota(jnp.int32, (slots, slots), 1)
    span = 2 * nz
    by_device = (
        from_row == ((to_row % span) // 2) * (2 * n_plane) + (to_row % 2) * n_plane + to_row // span
    ).astype(BF)
    by_plane = (
        to_row == ((from_row % span) // 2) * (2 * n_plane) + (from_row % 2) * n_plane + from_row // span
    ).astype(BF)

    weight_copies[0].wait()
    weight_copies[1].wait()
    acc_g[...] = jnp.zeros_like(acc_g)
    acc_u[...] = jnp.zeros_like(acc_u)

    def spread(j, carry):
        done(zbuf.at[j, pl.ds(0, nz - 1)], send_z.at[j], recv_z.at[j], False)
        moved = dot_nn(by_device, zbuf[j].reshape(slots, cw)).astype(BF)
        xout[j] = moved.reshape(n_plane, span, cw)
        for d in range(1, n_plane):
            q_ = (q + d) % n_plane
            remote(xout.at[j, q_], xbuf.at[j, q], send_x.at[j], recv_x.at[j], plane_dev(q_)).start()
        xbuf[j, q] = xout[j, q]
        done(xbuf.at[j, pl.ds(0, n_plane - 1)], send_x.at[j], recv_x.at[j], False)
        arrived = xbuf[j].reshape(slots, cw)
        at = columns(j, cw)
        acc_g[...] += dot_nn(arrived, gate_v[at, :])
        acc_u[...] += dot_nn(arrived, up_v[at, :])
        return carry

    steps(0, CHUNKS, spread)

    for copy in weight_copies[2:]:
        copy.wait()
    gates = acc_g[...]
    hidden_v[...] = (gates / (1.0 + jnp.exp(-gates)) * acc_u[...]).astype(BF)

    def produce(j, carry):
        made = dot_nn(hidden_v[...], down_v[j]).astype(BF)
        yout[j] = made.reshape(n_plane, span, cw)
        for d in range(1, n_plane):
            q_ = (q + d) % n_plane
            remote(yout.at[j, q_], ybuf.at[j, q], send_rx.at[j], recv_rx.at[j], plane_dev(q_)).start()
        ybuf[j, q] = yout[j, q]
        return carry

    def give_back(j, carry):
        done(ybuf.at[j, pl.ds(0, n_plane - 1)], send_rx.at[j], recv_rx.at[j], False)
        moved = dot_nn(by_plane, ybuf[j].reshape(slots, cw)).astype(BF)
        zout[j] = moved.reshape(nz, 2 * n_plane, cw)
        for d in far:
            z_ = (z + d) % nz
            remote(zout.at[j, z_], rbuf.at[j, z], send_rz.at[j], recv_rz.at[j], dev(z_, c, x)).start()
        rbuf[j, z] = zout[j, z]
        return carry

    steps(0, CHUNKS, produce)
    steps(0, CHUNKS // 2, give_back)

    done(hbuf.at[:, pl.ds(0, nz - 1)], send_m.at[2], recv_m.at[2], False)
    share = nz * quarter
    qn_v[...] = rms(hbuf[0].reshape(share, hd), qgain_in[...])
    kvown[0] = rms(hbuf[1].reshape(share, hd), kgain_in[...]).reshape(nz, quarter, hd)
    kvown[1] = hbuf[2]
    for d in range(1, n_plane):
        q_ = (q + d) % n_plane
        remote(kvown, kvbuf.at[:, :, c, x], send_m.at[4], recv_m.at[4], plane_dev(q_)).start()
    for i in range(2):
        kvbuf[i, :, c, x] = kvown[i]
    others = kvbuf.at[:, pl.ds(0, nz * (n_plane - 1) // n_plane)]
    done(fcbuf.at[pl.ds(0, nx - 1)], send_m.at[1], recv_m.at[1], False)
    bias = fcbuf[z // heads, pl.ds(z % heads, 1), :]
    scale = hd ** (-0.5)
    done(others, send_m.at[4], recv_m.at[4], False)
    key_at = lax.broadcasted_iota(jnp.int32, (rows, length), 1)
    block = lax.broadcasted_iota(jnp.int32, (rows, 1), 0)

    def attend(b, carry):
        mine_at = block + b * rows
        query_at = ((mine_at // quarter) * CORES + c) * rows + x * quarter + mine_at % quarter
        keys = kvbuf[0].reshape(length, hd)
        scores = dot_nt(qn_v[pl.ds(pl.multiple_of(b * rows, rows), rows), :], keys) * scale - bias
        scores = jnp.where(key_at <= query_at, scores, -1e30)
        scores_v[...] = scores
        best = jnp.max(scores, axis=1, keepdims=True)
        weights = jnp.exp(scores_v[...] - best)
        below = jnp.sum(weights, axis=1, keepdims=True)
        mixed = dot_nn(weights.astype(BF), kvbuf[1].reshape(length, hd)) / below
        per = rows // quarter
        o_v[pl.ds(b * per, per)] = mixed.astype(BF).reshape(per, quarter, hd)
        return carry

    steps(0, share // rows, attend)
    for d in far:
        z_ = (z + d) % nz
        remote(o_v.at[z_], obuf.at[z], send_m.at[5], recv_m.at[5], dev(z_, c, x)).start()
    obuf[z] = o_v[z]

    steps(CHUNKS // 2, CHUNKS, give_back)

    def combine(j, carry):
        done(rbuf.at[j, pl.ds(0, nz - 1)], send_rz.at[j], recv_rz.at[j], False)
        got = rbuf[j].reshape(slots, cw)
        routed = dot_nn(mix_v[0], got) + dot_nn(mix_v[1], got) + dot_nn(mix_v[2], got)
        at = columns(j, cw)
        made_v[:, at] = (sh_v[j].astype(F32) + routed).astype(BF)
        pltpu.make_async_copy(made_v.at[:, at], rout_out.at[:, at], outsem.at[j]).start()
        return carry

    steps(0, CHUNKS // 2, combine)

    done(obuf.at[pl.ds(0, nz - 1)], send_m.at[5], recv_m.at[5], False)
    for d in range(1, nx):
        x_ = (x + d) % nx
        remote(
            obuf.at[pl.ds(x_ * heads, heads)], fbuf.at[x], send_m.at[6], recv_m.at[6], dev(z, c, x_)
        ).start()
    fbuf[x] = obuf[pl.ds(x * heads, heads)]

    steps(CHUNKS // 2, CHUNKS - 1, combine)
    done(fbuf.at[pl.ds(0, nx - 1)], send_m.at[6], recv_m.at[6], False)
    for x_ in range(nx):
        att_out[x_ * block_rows : (x_ + 1) * block_rows, :] = dot_nn(
            by_position, fbuf[x_].reshape(block_rows, hd)
        ).astype(BF)
    steps(CHUNKS - 1, CHUNKS, combine)


    def drain(j, carry):
        at = columns(j, cw)
        pltpu.make_async_copy(made_v.at[:, at], rout_out.at[:, at], outsem.at[j]).wait()
        done(zbuf.at[j, pl.ds(0, nz - 1)], send_z.at[j], recv_z.at[j], True)
        done(xbuf.at[j, pl.ds(0, n_plane - 1)], send_x.at[j], recv_x.at[j], True)
        done(ybuf.at[j, pl.ds(0, n_plane - 1)], send_rx.at[j], recv_rx.at[j], True)
        done(rbuf.at[j, pl.ds(0, nz - 1)], send_rz.at[j], recv_rz.at[j], True)
        return carry

    steps(0, CHUNKS, drain)
    done(s1raw.at[pl.ds(0, nx - 1)], send_m.at[0], recv_m.at[0], True)
    done(fcbuf.at[pl.ds(0, nx - 1)], send_m.at[1], recv_m.at[1], True)
    done(hbuf.at[:, pl.ds(0, nz - 1)], send_m.at[2], recv_m.at[2], True)
    done(shbuf.at[pl.ds(0, nx - 1)], send_m.at[3], recv_m.at[3], True)
    done(others, send_m.at[4], recv_m.at[4], True)
    done(obuf.at[pl.ds(0, nz - 1)], send_m.at[5], recv_m.at[5], True)
    done(fbuf.at[pl.ds(0, nx - 1)], send_m.at[6], recv_m.at[6], True)


def solution(mesh):
    nx = mesh.shape["tp"]
    nz = mesh.shape["ep"] // CORES

    def local(
        queries,
        key_vectors,
        values,
        forget_cum,
        query_gain,
        key_gain,
        tokens,
        norm_gain,
        routes,
        route_weights,
        expert_gate,
        expert_up,
        expert_down,
        shared_gate,
        shared_up,
        shared_down,
    ):
        rows, heads, hd = queries.shape
        width = tokens.shape[1]
        hidden = expert_gate.shape[2]
        part = shared_down.shape[0]
        length = forget_cum.shape[0]
        n_plane = CORES * nx
        slots = nz * n_plane * 2
        cw = width // CHUNKS
        quarter = rows // nx
        share = nz * quarter
        vm = pl.BlockSpec(memory_space=pltpu.VMEM)
        hbm = pl.BlockSpec(memory_space=pltpu.HBM)
        V = pltpu.VMEM
        by_plane = V((CHUNKS, nz, 2 * n_plane, cw), BF)
        by_device = V((CHUNKS, n_plane, 2 * nz, cw), BF)
        dma = pltpu.SemaphoreType.DMA
        att, out = pl.pallas_call(
            functools.partial(kernel, nz, nx),
            out_shape=(
                jax.ShapeDtypeStruct((rows * heads, hd), BF),
                jax.ShapeDtypeStruct((rows, width), BF),
            ),
            in_specs=[hbm] * 16,
            out_specs=(vm, hbm),
            scratch_shapes=[
                V((rows, width), BF),
                dma((CHUNKS,)),
                V((width, hidden), BF),
                V((width, hidden), BF),
                V((CHUNKS, hidden, cw), BF),
                V((CHUNKS, rows, cw), BF),
                by_plane,
                by_plane,
                by_device,
                by_device,
                by_device,
                by_device,
                by_plane,
                by_plane,
                V((slots, rows), BF),
                V((3, rows, slots), BF),
                V((slots, hidden), F32),
                V((slots, hidden), F32),
                V((slots, hidden), BF),
                V((nx, 3, part, width), BF),
                V((CHUNKS, rows, cw), BF),
                V((nx, heads, length), F32),
                V((heads, length), F32),
                V((1, hd), F32),
                V((1, hd), F32),
                V((1, width), F32),
                V((2, rows), jnp.int32),
                V((2, rows), F32),
                V((rows, width), BF),
                V((3, rows * heads, hd), BF),
                V((nx, 3, quarter * heads, hd), BF),
                V((3, nz, quarter, hd), BF),
                V((3, nz, quarter, hd), BF),
                V((2, nz, CORES, nx, quarter, hd), BF),
                V((share, hd), BF),
                V((2, nz, quarter, hd), BF),
                V((rows, length), F32),
                V((nz, quarter, hd), BF),
                V((nz, quarter, hd), BF),
                V((nx, heads, quarter, hd), BF),
                dma((2 + CHUNKS,)),
                dma((13,)),
            ]
            + [dma((CHUNKS,))] * 8
            + [dma((7,))] * 2,
            compiler_params=pltpu.CompilerParams(
                collective_id=0, has_side_effects=True, vmem_limit_bytes=VLIM * 1024 * 1024
            ),
        )(
            queries.reshape(rows * heads, hd),
            key_vectors.reshape(rows * heads, hd),
            values.reshape(rows * heads, hd),
            forget_cum.T,
            query_gain.reshape(1, hd),
            key_gain.reshape(1, hd),
            tokens,
            norm_gain.reshape(1, width),
            routes.T,
            route_weights.T,
            shared_gate.T,
            shared_up.T,
            shared_down,
            expert_gate,
            expert_up,
            expert_down,
        )
        return att.reshape(rows, heads, hd), out

    placed = (
        P(("grp", "ep"), "tp", None),
        P(("grp", "ep"), "tp", None),
        P(("grp", "ep"), "tp", None),
        P("grp", "tp"),
        P(),
        P(),
        P(("grp", "ep", "tp"), None),
        P(),
        P(("grp", "ep", "tp"), None),
        P(("grp", "ep", "tp"), None),
        P(("ep", "tp"), None, None),
        P(("ep", "tp"), None, None),
        P(("ep", "tp"), None, None),
        P(None, "tp"),
        P(None, "tp"),
        P("tp", None),
    )
    return jax.shard_map(
        local,
        mesh=mesh,
        in_specs=placed,
        out_specs=(P(("grp", "ep"), "tp", None), P(("grp", "ep", "tp"), None)),
        check_vma=False,
    )
```

```python
import functools

import jax
import jax.numpy as jnp
from jax import lax
from jax.experimental import pallas as pl
from jax.experimental.pallas import tpu as pltpu
from jax.sharding import PartitionSpec as P

MESH = pl.DeviceIdType.MESH
CORES = 2
CHUNKS = 4
VLIM = 63
BF = jnp.bfloat16
F32 = jnp.float32


def columns(j, size):
    return pl.ds(j * size if isinstance(j, int) else pl.multiple_of(j * size, size), size)


def steps(first, last, body):
    if last - first == 1:
        body(first, 0)
    else:
        lax.fori_loop(first, last, body, 0)


def dot_nn(a, b):
    return lax.dot_general(a, b, (((1,), (0,)), ((), ())), preferred_element_type=F32)


def dot_nt(a, b):
    return lax.dot_general(a, b, (((1,), (1,)), ((), ())), preferred_element_type=F32)


def rms(values, gain):
    wide = values.astype(F32)
    inverse = lax.rsqrt(jnp.mean(wide * wide, axis=-1, keepdims=True) + 1e-06)
    return (wide * inverse * gain).astype(BF)


def kernel(
    nz,
    nx,
    q_hbm,
    k_hbm,
    v_hbm,
    fc_hbm,
    qgain_hbm,
    kgain_hbm,
    tokens_hbm,
    ngain_hbm,
    routes_hbm,
    weights_hbm,
    sgate_hbm,
    sup_hbm,
    sdown_hbm,
    gate_hbm,
    up_hbm,
    down_hbm,
    att_out,
    rout_out,
    made_v,
    outsem,
    gate_v,
    up_v,
    down_v,
    normed_v,
    outgoing,
    zbuf,
    xout,
    xbuf,
    yout,
    ybuf,
    zout,
    rbuf,
    sel_v,
    mix_v,
    acc_g,
    acc_u,
    hidden_v,
    shbuf,
    sh_v,
    fcbuf,
    fc_in,
    qgain_in,
    kgain_in,
    ngain_in,
    routes_in,
    weights_in,
    tokens_in,
    qkv_in,
    s1raw,
    s1,
    hbuf,
    kvbuf,
    qn_v,
    kvown,
    scores_v,
    o_v,
    obuf,
    fbuf,
    wsem,
    osem,
    send_z,
    recv_z,
    send_x,
    recv_x,
    send_rx,
    recv_rx,
    send_rz,
    recv_rz,
    send_m,
    recv_m,
):
    n_plane = CORES * nx
    rows = tokens_hbm.shape[0]
    width = tokens_hbm.shape[1]
    cw = width // CHUNKS
    slots = nz * n_plane * 2
    quarter = rows // nx
    hd = qgain_hbm.shape[1]
    heads = q_hbm.shape[0] // rows
    length = nz * CORES * rows

    ep = lax.axis_index("ep")
    x = lax.axis_index("tp")
    z = ep // CORES
    c = ep % CORES
    q = c * nx + x

    def dev(z_, c_, x_):
        return {"ep": z_ * CORES + c_, "tp": x_}

    def plane_dev(q_):
        return dev(z, q_ // nx, q_ % nx)

    far = []
    for d in range(nz // 2, 0, -1):
        far.append(d)
        if 2 * d != nz:
            far.append(nz - d)

    def remote(src, dst, s_sem, r_sem, device):
        return pltpu.make_async_remote_copy(
            src_ref=src, dst_ref=dst, send_sem=s_sem, recv_sem=r_sem, device_id=device, device_id_type=MESH
        )

    def done(ref, s_sem, r_sem, sent):
        copy = remote(ref, ref, s_sem, r_sem, dev(z, c, x))
        if sent:
            copy.wait_send()
        else:
            copy.wait_recv()

    barrier = pltpu.get_barrier_semaphore()
    for d in far:
        pl.semaphore_signal(barrier, inc=1, device_id=dev((z + d) % nz, c, x), device_id_type=MESH)
    for d in range(1, n_plane):
        pl.semaphore_signal(barrier, inc=1, device_id=plane_dev((q + d) % n_plane), device_id_type=MESH)

    token_copy = pltpu.make_async_copy(tokens_hbm, tokens_in, osem.at[0])
    token_copy.start()
    own_copies = [
        pltpu.make_async_copy(ref, qkv_in.at[i], osem.at[1 + i]) for i, ref in enumerate((q_hbm, k_hbm, v_hbm))
    ] + [
        pltpu.make_async_copy(ref, shbuf.at[x, i], osem.at[4 + i])
        for i, ref in enumerate((sgate_hbm, sup_hbm, sdown_hbm))
    ]
    small_copies = [
        pltpu.make_async_copy(src, dst, osem.at[7 + i])
        for i, (src, dst) in enumerate(
            (
                (routes_hbm, routes_in),
                (weights_hbm, weights_in),
                (ngain_hbm, ngain_in),
                (qgain_hbm, qgain_in),
                (kgain_hbm, kgain_in),
                (fc_hbm, fc_in),
            )
        )
    ]
    for copy in small_copies + own_copies:
        copy.start()
    weight_copies = [
        pltpu.make_async_copy(gate_hbm.at[0], gate_v, wsem.at[0]),
        pltpu.make_async_copy(up_hbm.at[0], up_v, wsem.at[1]),
    ] + [
        pltpu.make_async_copy(down_hbm.at[0, :, pl.ds(j * cw, cw)], down_v.at[j], wsem.at[2 + j])
        for j in range(CHUNKS)
    ]
    for copy in weight_copies:
        copy.start()

    for copy in small_copies:
        copy.wait()

    slot = lax.broadcasted_iota(jnp.int32, (slots, rows), 0)
    expert = (slot // (2 * n_plane)) * n_plane + slot % n_plane
    copy_of = (slot // n_plane) % 2
    first = (routes_in[0:1, :] == expert).astype(F32)
    second = (routes_in[1:2, :] == expert).astype(F32)
    named = first + second
    earlier = (
        lax.broadcasted_iota(jnp.int32, (rows, rows), 0) < lax.broadcasted_iota(jnp.int32, (rows, rows), 1)
    ).astype(BF)
    rank = dot_nn(named.astype(BF), earlier)
    mine = jnp.where(rank == copy_of.astype(F32), 1.0, 0.0)
    sel_v[...] = (named * mine).astype(BF)
    token_copy.wait()
    total = jnp.zeros((rows, 1), F32)
    for j in range(CHUNKS):
        part = tokens_in[:, j * cw : (j + 1) * cw].astype(F32)
        total = total + jnp.sum(part * part, axis=-1, keepdims=True)
    inverse = lax.rsqrt(total / width + 1e-06)

    pl.semaphore_wait(barrier, len(far) + n_plane - 1)

    def dispatch(j, carry):
        at = columns(j, cw)
        part = (tokens_in[:, at].astype(F32) * inverse * ngain_in[:, at]).astype(BF)
        normed_v[j] = part
        picked = dot_nn(sel_v[...], part).astype(BF)
        outgoing[j] = picked.reshape(nz, 2 * n_plane, cw)
        for d in far:
            z_ = (z + d) % nz
            remote(outgoing.at[j, z_], zbuf.at[j, z], send_z.at[j], recv_z.at[j], dev(z_, c, x)).start()
        zbuf[j, z] = outgoing[j, z]
        return carry

    steps(0, 1, dispatch)

    block_rows = quarter * heads
    for copy in own_copies[:3]:
        copy.wait()
    for d in range(1, nx):
        x_ = (x + d) % nx
        remote(
            qkv_in.at[:, pl.ds(pl.multiple_of(x_ * block_rows, block_rows), block_rows)],
            s1raw.at[x],
            send_m.at[0],
            recv_m.at[0],
            dev(z, c, x_),
        ).start()
        remote(fc_in, fcbuf.at[x], send_m.at[1], recv_m.at[1], dev(z, c, x_)).start()
    s1raw[x] = qkv_in[:, pl.ds(pl.multiple_of(x * block_rows, block_rows), block_rows)]
    fcbuf[x] = fc_in[...]

    steps(1, 2, dispatch)

    mix = (mine * (first * weights_in[0:1, :] + second * weights_in[1:2, :])).T
    high = mix.astype(BF)
    left = mix - high.astype(F32)
    middle = left.astype(BF)
    mix_v[0] = high
    mix_v[1] = middle
    mix_v[2] = (left - middle.astype(F32)).astype(BF)

    by_head_to = lax.broadcasted_iota(jnp.int32, (block_rows, block_rows), 0)
    by_head_from = lax.broadcasted_iota(jnp.int32, (block_rows, block_rows), 1)
    by_head = (by_head_from == (by_head_to % quarter) * heads + by_head_to // quarter).astype(BF)
    by_position = (by_head_to == (by_head_from % quarter) * heads + by_head_from // quarter).astype(BF)
    done(s1raw.at[pl.ds(0, nx - 1)], send_m.at[0], recv_m.at[0], False)
    for x_ in range(nx):
        for i in range(3):
            s1[i, x_ * heads : (x_ + 1) * heads] = (
                dot_nn(by_head, s1raw[x_, i]).astype(BF).reshape(heads, quarter, hd)
            )

    def swap():
        for d in far:
            z_ = (z + d) % nz
            remote(s1.at[:, z_], hbuf.at[:, z], send_m.at[2], recv_m.at[2], dev(z_, c, x)).start()
        for i in range(3):
            hbuf[i, z] = s1[i, z]

    for copy in own_copies[3:]:
        copy.wait()
    for d in range(1, nx):
        remote(shbuf.at[x], shbuf.at[x], send_m.at[3], recv_m.at[3], dev(z, c, (x + d) % nx)).start()

    def shared():
        done(shbuf.at[pl.ds(0, nx - 1)], send_m.at[3], recv_m.at[3], False)

        hiddens = []
        for n in range(nx):
            gate_sum = jnp.zeros((rows, sgate_hbm.shape[0]), F32)
            up_sum = jnp.zeros((rows, sgate_hbm.shape[0]), F32)
            for j in range(CHUNKS):
                gate_sum = gate_sum + dot_nt(normed_v[j], shbuf[n, 0, :, j * cw : (j + 1) * cw])
                up_sum = up_sum + dot_nt(normed_v[j], shbuf[n, 1, :, j * cw : (j + 1) * cw])
            hiddens.append((gate_sum / (1.0 + jnp.exp(-gate_sum)) * up_sum).astype(BF))

        def shared_down(j, carry):
            at = columns(j, cw)
            out = jnp.zeros((rows, cw), F32)
            for n in range(nx):
                out = out + dot_nn(hiddens[n], shbuf[n, 2, :, at]).astype(BF).astype(F32)
            sh_v[j] = out.astype(BF)
            return carry

        steps(0, CHUNKS, shared_down)

    to_row = lax.broadcasted_iota(jnp.int32, (slots, slots), 0)
    from_row = lax.broadcasted_iota(jnp.int32, (slots, slots), 1)
    span = 2 * nz
    by_device = (
        from_row == ((to_row % span) // 2) * (2 * n_plane) + (to_row % 2) * n_plane + to_row // span
    ).astype(BF)
    by_plane = (
        to_row == ((from_row % span) // 2) * (2 * n_plane) + (from_row % 2) * n_plane + from_row // span
    ).astype(BF)

    weight_copies[0].wait()
    weight_copies[1].wait()
    acc_g[...] = jnp.zeros_like(acc_g)
    acc_u[...] = jnp.zeros_like(acc_u)

    def spread(j, carry):
        done(zbuf.at[j, pl.ds(0, nz - 1)], send_z.at[j], recv_z.at[j], False)
        moved = dot_nn(by_device, zbuf[j].reshape(slots, cw)).astype(BF)
        xout[j] = moved.reshape(n_plane, span, cw)
        for d in range(1, n_plane):
            q_ = (q + d) % n_plane
            remote(xout.at[j, q_], xbuf.at[j, q], send_x.at[j], recv_x.at[j], plane_dev(q_)).start()
        xbuf[j, q] = xout[j, q]
        return carry

    def absorb(j, carry):
        done(xbuf.at[j, pl.ds(0, n_plane - 1)], send_x.at[j], recv_x.at[j], False)
        arrived = xbuf[j].reshape(slots, cw)
        at = columns(j, cw)
        acc_g[...] += dot_nn(arrived, gate_v[at, :])
        acc_u[...] += dot_nn(arrived, up_v[at, :])
        return carry

    for j in range(CHUNKS):
        spread(j, 0)
        if j + 2 < CHUNKS:
            dispatch(j + 2, 0)
        if j == CHUNKS - 2:
            swap()
        if j:
            absorb(j - 1, 0)
        if j == CHUNKS - 2:
            shared()
    absorb(CHUNKS - 1, 0)

    for copy in weight_copies[2:]:
        copy.wait()
    gates = acc_g[...]
    hidden_v[...] = (gates / (1.0 + jnp.exp(-gates)) * acc_u[...]).astype(BF)

    def produce(j, carry):
        made = dot_nn(hidden_v[...], down_v[j]).astype(BF)
        yout[j] = made.reshape(n_plane, span, cw)
        for d in range(1, n_plane):
            q_ = (q + d) % n_plane
            remote(yout.at[j, q_], ybuf.at[j, q], send_rx.at[j], recv_rx.at[j], plane_dev(q_)).start()
        ybuf[j, q] = yout[j, q]
        return carry

    def give_back(j, carry):
        done(ybuf.at[j, pl.ds(0, n_plane - 1)], send_rx.at[j], recv_rx.at[j], False)
        moved = dot_nn(by_plane, ybuf[j].reshape(slots, cw)).astype(BF)
        zout[j] = moved.reshape(nz, 2 * n_plane, cw)
        for d in far:
            z_ = (z + d) % nz
            remote(zout.at[j, z_], rbuf.at[j, z], send_rz.at[j], recv_rz.at[j], dev(z_, c, x)).start()
        rbuf[j, z] = zout[j, z]
        return carry

    steps(0, CHUNKS, produce)
    steps(0, CHUNKS // 2, give_back)

    done(hbuf.at[:, pl.ds(0, nz - 1)], send_m.at[2], recv_m.at[2], False)
    share = nz * quarter
    qn_v[...] = rms(hbuf[0].reshape(share, hd), qgain_in[...])
    kvown[0] = rms(hbuf[1].reshape(share, hd), kgain_in[...]).reshape(nz, quarter, hd)
    kvown[1] = hbuf[2]
    for d in range(1, n_plane):
        q_ = (q + d) % n_plane
        remote(kvown, kvbuf.at[:, :, c, x], send_m.at[4], recv_m.at[4], plane_dev(q_)).start()
    for i in range(2):
        kvbuf[i, :, c, x] = kvown[i]
    others = kvbuf.at[:, pl.ds(0, nz * (n_plane - 1) // n_plane)]
    done(fcbuf.at[pl.ds(0, nx - 1)], send_m.at[1], recv_m.at[1], False)
    bias = fcbuf[z // heads, pl.ds(z % heads, 1), :]
    scale = hd ** (-0.5)
    done(others, send_m.at[4], recv_m.at[4], False)
    key_at = lax.broadcasted_iota(jnp.int32, (rows, length), 1)
    block = lax.broadcasted_iota(jnp.int32, (rows, 1), 0)

    def attend(b, carry):
        mine_at = block + b * rows
        query_at = ((mine_at // quarter) * CORES + c) * rows + x * quarter + mine_at % quarter
        keys = kvbuf[0].reshape(length, hd)
        scores = dot_nt(qn_v[pl.ds(pl.multiple_of(b * rows, rows), rows), :], keys) * scale - bias
        scores = jnp.where(key_at <= query_at, scores, -1e30)
        scores_v[...] = scores
        best = jnp.max(scores, axis=1, keepdims=True)
        weights = jnp.exp(scores_v[...] - best)
        below = jnp.sum(weights, axis=1, keepdims=True)
        mixed = dot_nn(weights.astype(BF), kvbuf[1].reshape(length, hd)) / below
        per = rows // quarter
        o_v[pl.ds(b * per, per)] = mixed.astype(BF).reshape(per, quarter, hd)
        return carry

    steps(0, share // rows, attend)
    for d in far:
        z_ = (z + d) % nz
        remote(o_v.at[z_], obuf.at[z], send_m.at[5], recv_m.at[5], dev(z_, c, x)).start()
    obuf[z] = o_v[z]


    def combine(j, carry):
        done(rbuf.at[j, pl.ds(0, nz - 1)], send_rz.at[j], recv_rz.at[j], False)
        got = rbuf[j].reshape(slots, cw)
        routed = dot_nn(mix_v[0], got) + dot_nn(mix_v[1], got) + dot_nn(mix_v[2], got)
        at = columns(j, cw)
        made_v[:, at] = (sh_v[j].astype(F32) + routed).astype(BF)
        pltpu.make_async_copy(made_v.at[:, at], rout_out.at[:, at], outsem.at[j]).start()
        return carry

    steps(0, 1, combine)
    steps(2, 3, give_back)
    steps(1, 2, combine)
    steps(3, CHUNKS, give_back)

    done(obuf.at[pl.ds(0, nz - 1)], send_m.at[5], recv_m.at[5], False)
    for d in range(1, nx):
        x_ = (x + d) % nx
        remote(
            obuf.at[pl.ds(x_ * heads, heads)], fbuf.at[x], send_m.at[6], recv_m.at[6], dev(z, c, x_)
        ).start()
    fbuf[x] = obuf[pl.ds(x * heads, heads)]

    steps(CHUNKS // 2, CHUNKS - 1, combine)
    done(fbuf.at[pl.ds(0, nx - 1)], send_m.at[6], recv_m.at[6], False)
    for x_ in range(nx):
        att_out[x_ * block_rows : (x_ + 1) * block_rows, :] = dot_nn(
            by_position, fbuf[x_].reshape(block_rows, hd)
        ).astype(BF)
    steps(CHUNKS - 1, CHUNKS, combine)


    def drain(j, carry):
        at = columns(j, cw)
        pltpu.make_async_copy(made_v.at[:, at], rout_out.at[:, at], outsem.at[j]).wait()
        done(zbuf.at[j, pl.ds(0, nz - 1)], send_z.at[j], recv_z.at[j], True)
        done(xbuf.at[j, pl.ds(0, n_plane - 1)], send_x.at[j], recv_x.at[j], True)
        done(ybuf.at[j, pl.ds(0, n_plane - 1)], send_rx.at[j], recv_rx.at[j], True)
        done(rbuf.at[j, pl.ds(0, nz - 1)], send_rz.at[j], recv_rz.at[j], True)
        return carry

    steps(0, CHUNKS, drain)
    done(s1raw.at[pl.ds(0, nx - 1)], send_m.at[0], recv_m.at[0], True)
    done(fcbuf.at[pl.ds(0, nx - 1)], send_m.at[1], recv_m.at[1], True)
    done(hbuf.at[:, pl.ds(0, nz - 1)], send_m.at[2], recv_m.at[2], True)
    done(shbuf.at[pl.ds(0, nx - 1)], send_m.at[3], recv_m.at[3], True)
    done(others, send_m.at[4], recv_m.at[4], True)
    done(obuf.at[pl.ds(0, nz - 1)], send_m.at[5], recv_m.at[5], True)
    done(fbuf.at[pl.ds(0, nx - 1)], send_m.at[6], recv_m.at[6], True)


def place_kernel(att_in, out_in, att_out, out_out, att_v, out_v, in_sem, out_sem):
    width = out_in.shape[1] // CHUNKS
    pieces = [(att_in, att_v, att_out)] + [
        (out_in.at[:, columns(j, width)], out_v.at[j], out_out.at[:, columns(j, width)]) for j in range(CHUNKS)
    ]
    ins = [pltpu.make_async_copy(a, v, in_sem.at[i]) for i, (a, v, b) in enumerate(pieces)]
    outs = [pltpu.make_async_copy(v, b, out_sem.at[i]) for i, (a, v, b) in enumerate(pieces)]
    for copy in ins:
        copy.start()
    for copy, after in zip(ins, outs):
        copy.wait()
        after.start()
    for copy in outs:
        copy.wait()


def place(att, out):
    outside = pl.BlockSpec(memory_space=pl.ANY)
    return pl.pallas_call(
        place_kernel,
        out_shape=(jax.ShapeDtypeStruct(att.shape, att.dtype), jax.ShapeDtypeStruct(out.shape, out.dtype)),
        in_specs=[outside, outside],
        out_specs=(outside, outside),
        scratch_shapes=[
            pltpu.VMEM(att.shape, att.dtype),
            pltpu.VMEM((CHUNKS, out.shape[0], out.shape[1] // CHUNKS), out.dtype),
            pltpu.SemaphoreType.DMA((1 + CHUNKS,)),
            pltpu.SemaphoreType.DMA((1 + CHUNKS,)),
        ],
        compiler_params=pltpu.CompilerParams(vmem_limit_bytes=60 * 1024 * 1024),
    )(att, out)


def solution(mesh):
    nx = mesh.shape["tp"]
    nz = mesh.shape["ep"] // CORES

    def local(
        queries,
        key_vectors,
        values,
        forget_cum,
        query_gain,
        key_gain,
        tokens,
        norm_gain,
        routes,
        route_weights,
        expert_gate,
        expert_up,
        expert_down,
        shared_gate,
        shared_up,
        shared_down,
    ):
        rows, heads, hd = queries.shape
        width = tokens.shape[1]
        hidden = expert_gate.shape[2]
        part = shared_down.shape[0]
        length = forget_cum.shape[0]
        n_plane = CORES * nx
        slots = nz * n_plane * 2
        cw = width // CHUNKS
        quarter = rows // nx
        share = nz * quarter
        vm = pl.BlockSpec(memory_space=pltpu.VMEM)
        hbm = pl.BlockSpec(memory_space=pltpu.HBM)
        V = pltpu.VMEM
        by_plane = V((CHUNKS, nz, 2 * n_plane, cw), BF)
        by_device = V((CHUNKS, n_plane, 2 * nz, cw), BF)
        dma = pltpu.SemaphoreType.DMA
        att, out = pl.pallas_call(
            functools.partial(kernel, nz, nx),
            out_shape=(
                jax.ShapeDtypeStruct((rows * heads, hd), BF),
                jax.ShapeDtypeStruct((rows, width), BF),
            ),
            in_specs=[hbm] * 16,
            out_specs=(vm, hbm),
            scratch_shapes=[
                V((rows, width), BF),
                dma((CHUNKS,)),
                V((width, hidden), BF),
                V((width, hidden), BF),
                V((CHUNKS, hidden, cw), BF),
                V((CHUNKS, rows, cw), BF),
                by_plane,
                by_plane,
                by_device,
                by_device,
                by_device,
                by_device,
                by_plane,
                by_plane,
                V((slots, rows), BF),
                V((3, rows, slots), BF),
                V((slots, hidden), F32),
                V((slots, hidden), F32),
                V((slots, hidden), BF),
                V((nx, 3, part, width), BF),
                V((CHUNKS, rows, cw), BF),
                V((nx, heads, length), F32),
                V((heads, length), F32),
                V((1, hd), F32),
                V((1, hd), F32),
                V((1, width), F32),
                V((2, rows), jnp.int32),
                V((2, rows), F32),
                V((rows, width), BF),
                V((3, rows * heads, hd), BF),
                V((nx, 3, quarter * heads, hd), BF),
                V((3, nz, quarter, hd), BF),
                V((3, nz, quarter, hd), BF),
                V((2, nz, CORES, nx, quarter, hd), BF),
                V((share, hd), BF),
                V((2, nz, quarter, hd), BF),
                V((rows, length), F32),
                V((nz, quarter, hd), BF),
                V((nz, quarter, hd), BF),
                V((nx, heads, quarter, hd), BF),
                dma((2 + CHUNKS,)),
                dma((13,)),
            ]
            + [dma((CHUNKS,))] * 8
            + [dma((7,))] * 2,
            compiler_params=pltpu.CompilerParams(
                collective_id=0, has_side_effects=True, vmem_limit_bytes=VLIM * 1024 * 1024
            ),
        )(
            queries.reshape(rows * heads, hd),
            key_vectors.reshape(rows * heads, hd),
            values.reshape(rows * heads, hd),
            forget_cum.T,
            query_gain.reshape(1, hd),
            key_gain.reshape(1, hd),
            tokens,
            norm_gain.reshape(1, width),
            routes.T,
            route_weights.T,
            shared_gate.T,
            shared_up.T,
            shared_down,
            expert_gate,
            expert_up,
            expert_down,
        )
        return place(att.reshape(rows, heads, hd), out)

    placed = (
        P(("grp", "ep"), "tp", None),
        P(("grp", "ep"), "tp", None),
        P(("grp", "ep"), "tp", None),
        P("grp", "tp"),
        P(),
        P(),
        P(("grp", "ep", "tp"), None),
        P(),
        P(("grp", "ep", "tp"), None),
        P(("grp", "ep", "tp"), None),
        P(("ep", "tp"), None, None),
        P(("ep", "tp"), None, None),
        P(("ep", "tp"), None, None),
        P(None, "tp"),
        P(None, "tp"),
        P("tp", None),
    )
    return jax.shard_map(
        local,
        mesh=mesh,
        in_specs=placed,
        out_specs=(P(("grp", "ep"), "tp", None), P(("grp", "ep", "tp"), None)),
        check_vma=False,
    )
```

```python
import functools

import jax
import jax.numpy as jnp
from jax import lax
from jax.experimental import pallas as pl
from jax.experimental.pallas import tpu as pltpu
from jax.sharding import PartitionSpec as P

MESH = pl.DeviceIdType.MESH
CORES = 2
CHUNKS = 4
VLIM_KIB = 52000
BF = jnp.bfloat16
F32 = jnp.float32


def columns(j, size):
    return pl.ds(j * size if isinstance(j, int) else pl.multiple_of(j * size, size), size)


def steps(first, last, body):
    if last - first == 1:
        body(first, 0)
    else:
        lax.fori_loop(first, last, body, 0)


def dot_nn(a, b):
    return lax.dot_general(a, b, (((1,), (0,)), ((), ())), preferred_element_type=F32)


def dot_nt(a, b):
    return lax.dot_general(a, b, (((1,), (1,)), ((), ())), preferred_element_type=F32)


def rms(values, gain):
    wide = values.astype(F32)
    inverse = lax.rsqrt(jnp.mean(wide * wide, axis=-1, keepdims=True) + 1e-06)
    return (wide * inverse * gain).astype(BF)


def kernel(
    nz,
    nx,
    q_hbm,
    k_hbm,
    v_hbm,
    fc_hbm,
    qgain_hbm,
    kgain_hbm,
    tokens_hbm,
    ngain_hbm,
    routes_hbm,
    weights_hbm,
    sgate_hbm,
    sup_hbm,
    sdown_hbm,
    gate_hbm,
    up_hbm,
    down_hbm,
    att_out,
    rout_out,
    gate_v,
    up_v,
    down_v,
    normed_v,
    outgoing,
    zbuf,
    xout,
    xbuf,
    yout,
    ybuf,
    zout,
    rbuf,
    sel_v,
    mix_v,
    acc_g,
    acc_u,
    hidden_v,
    shbuf,
    sh_v,
    fcbuf,
    fc_in,
    qgain_in,
    kgain_in,
    ngain_in,
    routes_in,
    weights_in,
    tokens_in,
    qkv_in,
    s1raw,
    s1,
    hbuf,
    kvbuf,
    qn_v,
    kvown,
    scores_v,
    o_v,
    obuf,
    fbuf,
    wsem,
    osem,
    send_z,
    recv_z,
    send_x,
    recv_x,
    send_rx,
    recv_rx,
    send_rz,
    recv_rz,
    send_m,
    recv_m,
):
    n_plane = CORES * nx
    rows = tokens_hbm.shape[0]
    width = tokens_hbm.shape[1]
    cw = width // CHUNKS
    slots = nz * n_plane * 2
    quarter = rows // nx
    hd = qgain_hbm.shape[1]
    heads = q_hbm.shape[0] // rows
    length = nz * CORES * rows

    ep = lax.axis_index("ep")
    x = lax.axis_index("tp")
    z = ep // CORES
    c = ep % CORES
    q = c * nx + x

    def dev(z_, c_, x_):
        return {"ep": z_ * CORES + c_, "tp": x_}

    def plane_dev(q_):
        return dev(z, q_ // nx, q_ % nx)

    far = []
    for d in range(nz // 2, 0, -1):
        far.append(d)
        if 2 * d != nz:
            far.append(nz - d)

    def remote(src, dst, s_sem, r_sem, device):
        return pltpu.make_async_remote_copy(
            src_ref=src, dst_ref=dst, send_sem=s_sem, recv_sem=r_sem, device_id=device, device_id_type=MESH
        )

    def done(ref, s_sem, r_sem, sent):
        copy = remote(ref, ref, s_sem, r_sem, dev(z, c, x))
        if sent:
            copy.wait_send()
        else:
            copy.wait_recv()

    barrier = pltpu.get_barrier_semaphore()
    for d in far:
        pl.semaphore_signal(barrier, inc=1, device_id=dev((z + d) % nz, c, x), device_id_type=MESH)
    for d in range(1, n_plane):
        pl.semaphore_signal(barrier, inc=1, device_id=plane_dev((q + d) % n_plane), device_id_type=MESH)

    token_copy = pltpu.make_async_copy(tokens_hbm, tokens_in, osem.at[0])
    token_copy.start()
    own_copies = [
        pltpu.make_async_copy(ref, qkv_in.at[i], osem.at[1 + i]) for i, ref in enumerate((q_hbm, k_hbm, v_hbm))
    ] + [
        pltpu.make_async_copy(ref, shbuf.at[x, i], osem.at[4 + i])
        for i, ref in enumerate((sgate_hbm, sup_hbm, sdown_hbm))
    ]
    small_copies = [
        pltpu.make_async_copy(src, dst, osem.at[7 + i])
        for i, (src, dst) in enumerate(
            (
                (routes_hbm, routes_in),
                (weights_hbm, weights_in),
                (ngain_hbm, ngain_in),
                (qgain_hbm, qgain_in),
                (kgain_hbm, kgain_in),
                (fc_hbm, fc_in),
            )
        )
    ]
    for copy in small_copies + own_copies:
        copy.start()
    weight_copies = [
        pltpu.make_async_copy(gate_hbm.at[0], gate_v, wsem.at[0]),
        pltpu.make_async_copy(up_hbm.at[0], up_v, wsem.at[1]),
    ] + [
        pltpu.make_async_copy(down_hbm.at[0, :, pl.ds(j * cw, cw)], down_v.at[j], wsem.at[2 + j])
        for j in range(CHUNKS)
    ]
    for copy in weight_copies:
        copy.start()

    for copy in small_copies:
        copy.wait()

    slot = lax.broadcasted_iota(jnp.int32, (slots, rows), 0)
    expert = (slot // (2 * n_plane)) * n_plane + slot % n_plane
    copy_of = (slot // n_plane) % 2
    first = (routes_in[0:1, :] == expert).astype(F32)
    second = (routes_in[1:2, :] == expert).astype(F32)
    named = first + second
    earlier = (
        lax.broadcasted_iota(jnp.int32, (rows, rows), 0) < lax.broadcasted_iota(jnp.int32, (rows, rows), 1)
    ).astype(BF)
    rank = dot_nn(named.astype(BF), earlier)
    mine = jnp.where(rank == copy_of.astype(F32), 1.0, 0.0)
    sel_v[...] = (named * mine).astype(BF)
    token_copy.wait()
    total = jnp.zeros((rows, 1), F32)
    for j in range(CHUNKS):
        part = tokens_in[:, j * cw : (j + 1) * cw].astype(F32)
        total = total + jnp.sum(part * part, axis=-1, keepdims=True)
    inverse = lax.rsqrt(total / width + 1e-06)

    pl.semaphore_wait(barrier, len(far) + n_plane - 1)

    def dispatch(j, carry):
        at = columns(j, cw)
        part = (tokens_in[:, at].astype(F32) * inverse * ngain_in[:, at]).astype(BF)
        normed_v[j] = part
        picked = dot_nn(sel_v[...], part).astype(BF)
        outgoing[j] = picked.reshape(nz, 2 * n_plane, cw)
        for d in far:
            z_ = (z + d) % nz
            remote(outgoing.at[j, z_], zbuf.at[j, z], send_z.at[j], recv_z.at[j], dev(z_, c, x)).start()
        zbuf[j, z] = outgoing[j, z]
        return carry

    steps(0, 1, dispatch)

    block_rows = quarter * heads
    for copy in own_copies[:3]:
        copy.wait()
    for d in range(1, nx):
        x_ = (x + d) % nx
        remote(
            qkv_in.at[:, pl.ds(pl.multiple_of(x_ * block_rows, block_rows), block_rows)],
            s1raw.at[x],
            send_m.at[0],
            recv_m.at[0],
            dev(z, c, x_),
        ).start()
        remote(fc_in, fcbuf.at[x], send_m.at[1], recv_m.at[1], dev(z, c, x_)).start()
    s1raw[x] = qkv_in[:, pl.ds(pl.multiple_of(x * block_rows, block_rows), block_rows)]
    fcbuf[x] = fc_in[...]

    steps(1, 2, dispatch)

    mix = (mine * (first * weights_in[0:1, :] + second * weights_in[1:2, :])).T
    high = mix.astype(BF)
    left = mix - high.astype(F32)
    middle = left.astype(BF)
    mix_v[0] = high
    mix_v[1] = middle
    mix_v[2] = (left - middle.astype(F32)).astype(BF)

    by_head_to = lax.broadcasted_iota(jnp.int32, (block_rows, block_rows), 0)
    by_head_from = lax.broadcasted_iota(jnp.int32, (block_rows, block_rows), 1)
    by_head = (by_head_from == (by_head_to % quarter) * heads + by_head_to // quarter).astype(BF)
    by_position = (by_head_to == (by_head_from % quarter) * heads + by_head_from // quarter).astype(BF)
    done(s1raw.at[pl.ds(0, nx - 1)], send_m.at[0], recv_m.at[0], False)
    for x_ in range(nx):
        for i in range(3):
            s1[i, x_ * heads : (x_ + 1) * heads] = (
                dot_nn(by_head, s1raw[x_, i]).astype(BF).reshape(heads, quarter, hd)
            )

    def swap():
        for d in far:
            z_ = (z + d) % nz
            remote(s1.at[:, z_], hbuf.at[:, z], send_m.at[2], recv_m.at[2], dev(z_, c, x)).start()
        for i in range(3):
            hbuf[i, z] = s1[i, z]

    for copy in own_copies[3:]:
        copy.wait()
    for d in range(1, nx):
        remote(shbuf.at[x], shbuf.at[x], send_m.at[3], recv_m.at[3], dev(z, c, (x + d) % nx)).start()

    def shared():
        done(shbuf.at[pl.ds(0, nx - 1)], send_m.at[3], recv_m.at[3], False)

        hiddens = []
        for n in range(nx):
            gate_sum = jnp.zeros((rows, sgate_hbm.shape[0]), F32)
            up_sum = jnp.zeros((rows, sgate_hbm.shape[0]), F32)
            for j in range(CHUNKS):
                gate_sum = gate_sum + dot_nt(normed_v[j], shbuf[n, 0, :, j * cw : (j + 1) * cw])
                up_sum = up_sum + dot_nt(normed_v[j], shbuf[n, 1, :, j * cw : (j + 1) * cw])
            hiddens.append((gate_sum / (1.0 + jnp.exp(-gate_sum)) * up_sum).astype(BF))

        def shared_down(j, carry):
            at = columns(j, cw)
            out = jnp.zeros((rows, cw), F32)
            for n in range(nx):
                out = out + dot_nn(hiddens[n], shbuf[n, 2, :, at]).astype(BF).astype(F32)
            sh_v[j] = out.astype(BF)
            return carry

        steps(0, CHUNKS, shared_down)

    to_row = lax.broadcasted_iota(jnp.int32, (slots, slots), 0)
    from_row = lax.broadcasted_iota(jnp.int32, (slots, slots), 1)
    span = 2 * nz
    by_device = (
        from_row == ((to_row % span) // 2) * (2 * n_plane) + (to_row % 2) * n_plane + to_row // span
    ).astype(BF)
    by_plane = (
        to_row == ((from_row % span) // 2) * (2 * n_plane) + (from_row % 2) * n_plane + from_row // span
    ).astype(BF)

    weight_copies[0].wait()
    weight_copies[1].wait()
    acc_g[...] = jnp.zeros_like(acc_g)
    acc_u[...] = jnp.zeros_like(acc_u)

    def spread(j, carry):
        done(zbuf.at[j, pl.ds(0, nz - 1)], send_z.at[j], recv_z.at[j], False)
        moved = dot_nn(by_device, zbuf[j].reshape(slots, cw)).astype(BF)
        xout[j] = moved.reshape(n_plane, span, cw)
        for d in range(1, n_plane):
            q_ = (q + d) % n_plane
            remote(xout.at[j, q_], xbuf.at[j, q], send_x.at[j], recv_x.at[j], plane_dev(q_)).start()
        xbuf[j, q] = xout[j, q]
        return carry

    def absorb(j, carry):
        done(xbuf.at[j, pl.ds(0, n_plane - 1)], send_x.at[j], recv_x.at[j], False)
        arrived = xbuf[j].reshape(slots, cw)
        at = columns(j, cw)
        acc_g[...] += dot_nn(arrived, gate_v[at, :])
        acc_u[...] += dot_nn(arrived, up_v[at, :])
        return carry

    for j in range(CHUNKS):
        spread(j, 0)
        if j + 2 < CHUNKS:
            dispatch(j + 2, 0)
        if j == CHUNKS - 2:
            swap()
        if j:
            absorb(j - 1, 0)
        if j == CHUNKS - 2:
            shared()
    absorb(CHUNKS - 1, 0)

    for copy in weight_copies[2:]:
        copy.wait()
    gates = acc_g[...]
    hidden_v[...] = (gates / (1.0 + jnp.exp(-gates)) * acc_u[...]).astype(BF)

    def produce(j, carry):
        made = dot_nn(hidden_v[...], down_v[j]).astype(BF)
        yout[j] = made.reshape(n_plane, span, cw)
        for d in range(1, n_plane):
            q_ = (q + d) % n_plane
            remote(yout.at[j, q_], ybuf.at[j, q], send_rx.at[j], recv_rx.at[j], plane_dev(q_)).start()
        ybuf[j, q] = yout[j, q]
        return carry

    def give_back(j, carry):
        done(ybuf.at[j, pl.ds(0, n_plane - 1)], send_rx.at[j], recv_rx.at[j], False)
        moved = dot_nn(by_plane, ybuf[j].reshape(slots, cw)).astype(BF)
        zout[j] = moved.reshape(nz, 2 * n_plane, cw)
        for d in far:
            z_ = (z + d) % nz
            remote(zout.at[j, z_], rbuf.at[j, z], send_rz.at[j], recv_rz.at[j], dev(z_, c, x)).start()
        rbuf[j, z] = zout[j, z]
        return carry

    steps(0, CHUNKS, produce)
    steps(0, CHUNKS // 2, give_back)

    done(hbuf.at[:, pl.ds(0, nz - 1)], send_m.at[2], recv_m.at[2], False)
    share = nz * quarter
    qn_v[...] = rms(hbuf[0].reshape(share, hd), qgain_in[...])
    kvown[0] = rms(hbuf[1].reshape(share, hd), kgain_in[...]).reshape(nz, quarter, hd)
    kvown[1] = hbuf[2]
    for d in range(1, n_plane):
        q_ = (q + d) % n_plane
        remote(kvown, kvbuf.at[:, :, c, x], send_m.at[4], recv_m.at[4], plane_dev(q_)).start()
    for i in range(2):
        kvbuf[i, :, c, x] = kvown[i]
    others = kvbuf.at[:, pl.ds(0, nz * (n_plane - 1) // n_plane)]
    done(fcbuf.at[pl.ds(0, nx - 1)], send_m.at[1], recv_m.at[1], False)
    bias = fcbuf[z // heads, pl.ds(z % heads, 1), :]
    scale = hd ** (-0.5)
    done(others, send_m.at[4], recv_m.at[4], False)
    key_at = lax.broadcasted_iota(jnp.int32, (rows, length), 1)
    block = lax.broadcasted_iota(jnp.int32, (rows, 1), 0)

    def attend(b, carry):
        mine_at = block + b * rows
        query_at = ((mine_at // quarter) * CORES + c) * rows + x * quarter + mine_at % quarter
        keys = kvbuf[0].reshape(length, hd)
        scores = dot_nt(qn_v[pl.ds(pl.multiple_of(b * rows, rows), rows), :], keys) * scale - bias
        scores = jnp.where(key_at <= query_at, scores, -1e30)
        scores_v[...] = scores
        best = jnp.max(scores, axis=1, keepdims=True)
        weights = jnp.exp(scores_v[...] - best)
        below = jnp.sum(weights, axis=1, keepdims=True)
        mixed = dot_nn(weights.astype(BF), kvbuf[1].reshape(length, hd)) / below
        per = rows // quarter
        o_v[pl.ds(b * per, per)] = mixed.astype(BF).reshape(per, quarter, hd)
        return carry

    steps(0, share // rows, attend)
    for d in far:
        z_ = (z + d) % nz
        remote(o_v.at[z_], obuf.at[z], send_m.at[5], recv_m.at[5], dev(z_, c, x)).start()
    obuf[z] = o_v[z]

    def combine(j, carry):
        done(rbuf.at[j, pl.ds(0, nz - 1)], send_rz.at[j], recv_rz.at[j], False)
        got = rbuf[j].reshape(slots, cw)
        routed = dot_nn(mix_v[0], got) + dot_nn(mix_v[1], got) + dot_nn(mix_v[2], got)
        at = columns(j, cw)
        rout_out[:, at] = (sh_v[j].astype(F32) + routed).astype(BF)
        return carry

    steps(0, 1, combine)
    steps(2, 3, give_back)
    steps(1, 2, combine)
    steps(3, CHUNKS, give_back)

    done(obuf.at[pl.ds(0, nz - 1)], send_m.at[5], recv_m.at[5], False)
    for d in range(1, nx):
        x_ = (x + d) % nx
        remote(
            obuf.at[pl.ds(x_ * heads, heads)], fbuf.at[x], send_m.at[6], recv_m.at[6], dev(z, c, x_)
        ).start()
    fbuf[x] = obuf[pl.ds(x * heads, heads)]

    steps(CHUNKS // 2, CHUNKS - 1, combine)
    done(fbuf.at[pl.ds(0, nx - 1)], send_m.at[6], recv_m.at[6], False)
    for x_ in range(nx):
        att_out[x_ * block_rows : (x_ + 1) * block_rows, :] = dot_nn(
            by_position, fbuf[x_].reshape(block_rows, hd)
        ).astype(BF)
    steps(CHUNKS - 1, CHUNKS, combine)

    def drain(j, carry):
        done(zbuf.at[j, pl.ds(0, nz - 1)], send_z.at[j], recv_z.at[j], True)
        done(xbuf.at[j, pl.ds(0, n_plane - 1)], send_x.at[j], recv_x.at[j], True)
        done(ybuf.at[j, pl.ds(0, n_plane - 1)], send_rx.at[j], recv_rx.at[j], True)
        done(rbuf.at[j, pl.ds(0, nz - 1)], send_rz.at[j], recv_rz.at[j], True)
        return carry

    steps(0, CHUNKS, drain)
    done(s1raw.at[pl.ds(0, nx - 1)], send_m.at[0], recv_m.at[0], True)
    done(fcbuf.at[pl.ds(0, nx - 1)], send_m.at[1], recv_m.at[1], True)
    done(hbuf.at[:, pl.ds(0, nz - 1)], send_m.at[2], recv_m.at[2], True)
    done(shbuf.at[pl.ds(0, nx - 1)], send_m.at[3], recv_m.at[3], True)
    done(others, send_m.at[4], recv_m.at[4], True)
    done(obuf.at[pl.ds(0, nz - 1)], send_m.at[5], recv_m.at[5], True)
    done(fbuf.at[pl.ds(0, nx - 1)], send_m.at[6], recv_m.at[6], True)


def place_kernel(att_in, out_in, att_out, out_out, sems):
    copies = [
        pltpu.make_async_copy(att_in, att_out, sems.at[0]),
        pltpu.make_async_copy(out_in, out_out, sems.at[1]),
    ]
    for copy in copies:
        copy.start()
    for copy in copies:
        copy.wait()


def place(att, out):
    inside = pl.BlockSpec(memory_space=pltpu.VMEM)
    outside = pl.BlockSpec(memory_space=pl.ANY)
    return pl.pallas_call(
        place_kernel,
        out_shape=(jax.ShapeDtypeStruct(att.shape, att.dtype), jax.ShapeDtypeStruct(out.shape, out.dtype)),
        in_specs=[inside, inside],
        out_specs=(outside, outside),
        scratch_shapes=[pltpu.SemaphoreType.DMA((2,))],
        compiler_params=pltpu.CompilerParams(vmem_limit_bytes=VLIM_KIB * 1024),
    )(att, out)


def solution(mesh):
    nx = mesh.shape["tp"]
    nz = mesh.shape["ep"] // CORES

    def local(
        queries,
        key_vectors,
        values,
        forget_cum,
        query_gain,
        key_gain,
        tokens,
        norm_gain,
        routes,
        route_weights,
        expert_gate,
        expert_up,
        expert_down,
        shared_gate,
        shared_up,
        shared_down,
    ):
        rows, heads, hd = queries.shape
        width = tokens.shape[1]
        hidden = expert_gate.shape[2]
        part = shared_down.shape[0]
        length = forget_cum.shape[0]
        n_plane = CORES * nx
        slots = nz * n_plane * 2
        cw = width // CHUNKS
        quarter = rows // nx
        share = nz * quarter
        vm = pl.BlockSpec(memory_space=pltpu.VMEM)
        hbm = pl.BlockSpec(memory_space=pltpu.HBM)
        V = pltpu.VMEM
        by_plane = V((CHUNKS, nz, 2 * n_plane, cw), BF)
        by_device = V((CHUNKS, n_plane, 2 * nz, cw), BF)
        dma = pltpu.SemaphoreType.DMA
        att, out = pl.pallas_call(
            functools.partial(kernel, nz, nx),
            out_shape=(
                jax.ShapeDtypeStruct((rows * heads, hd), BF),
                jax.ShapeDtypeStruct((rows, width), BF),
            ),
            in_specs=[hbm] * 16,
            out_specs=(vm, vm),
            scratch_shapes=[
                V((width, hidden), BF),
                V((width, hidden), BF),
                V((CHUNKS, hidden, cw), BF),
                V((CHUNKS, rows, cw), BF),
                by_plane,
                by_plane,
                by_device,
                by_device,
                by_device,
                by_device,
                by_plane,
                by_plane,
                V((slots, rows), BF),
                V((3, rows, slots), BF),
                V((slots, hidden), F32),
                V((slots, hidden), F32),
                V((slots, hidden), BF),
                V((nx, 3, part, width), BF),
                V((CHUNKS, rows, cw), BF),
                V((nx, heads, length), F32),
                V((heads, length), F32),
                V((1, hd), F32),
                V((1, hd), F32),
                V((1, width), F32),
                V((2, rows), jnp.int32),
                V((2, rows), F32),
                V((rows, width), BF),
                V((3, rows * heads, hd), BF),
                V((nx, 3, quarter * heads, hd), BF),
                V((3, nz, quarter, hd), BF),
                V((3, nz, quarter, hd), BF),
                V((2, nz, CORES, nx, quarter, hd), BF),
                V((share, hd), BF),
                V((2, nz, quarter, hd), BF),
                V((rows, length), F32),
                V((nz, quarter, hd), BF),
                V((nz, quarter, hd), BF),
                V((nx, heads, quarter, hd), BF),
                dma((2 + CHUNKS,)),
                dma((13,)),
            ]
            + [dma((CHUNKS,))] * 8
            + [dma((7,))] * 2,
            compiler_params=pltpu.CompilerParams(
                collective_id=0, has_side_effects=True, vmem_limit_bytes=VLIM_KIB * 1024
            ),
        )(
            *(
                pltpu.with_memory_space_constraint(v, pltpu.HBM)
                for v in (
                    queries.reshape(rows * heads, hd),
                    key_vectors.reshape(rows * heads, hd),
                    values.reshape(rows * heads, hd),
                    forget_cum.T,
                    query_gain.reshape(1, hd),
                    key_gain.reshape(1, hd),
                    tokens,
                    norm_gain.reshape(1, width),
                    routes.T,
                    route_weights.T,
                    shared_gate.T,
                    shared_up.T,
                    shared_down,
                    expert_gate,
                    expert_up,
                    expert_down,
                )
            )
        )
        return place(att.reshape(rows, heads, hd), out)

    placed = (
        P(("grp", "ep"), "tp", None),
        P(("grp", "ep"), "tp", None),
        P(("grp", "ep"), "tp", None),
        P("grp", "tp"),
        P(),
        P(),
        P(("grp", "ep", "tp"), None),
        P(),
        P(("grp", "ep", "tp"), None),
        P(("grp", "ep", "tp"), None),
        P(("ep", "tp"), None, None),
        P(("ep", "tp"), None, None),
        P(("ep", "tp"), None, None),
        P(None, "tp"),
        P(None, "tp"),
        P("tp", None),
    )
    return jax.shard_map(
        local,
        mesh=mesh,
        in_specs=placed,
        out_specs=(P(("grp", "ep"), "tp", None), P(("grp", "ep", "tp"), None)),
        check_vma=False,
    )
```
